32 devices in a mesh: ep: 8 (over z, y), tp: 4 (over x, core).
Axes of the slice: x: 2, y: 2, z: 4, core: 2. Of those that a mesh axis runs over, the one named last changes fastest.
Arguments:
- mixer_microbatch: bfloat16 [8192, 2048], P(('ep', 'tp')), may hold values from -6 to 6
- mixer_gain_vector: float32 [2048], replicated, may hold values from 0.1 to 1.9
- asker_matrix: bfloat16 [2048, 1024], P(None, 'tp'), may hold values from -0.125 to 0.125
- matcher_matrix: bfloat16 [2048, 1024], P(None, 'tp'), may hold values from -0.125 to 0.125
- fading_matrix: bfloat16 [2048, 1024], P(None, 'tp'), may hold values from -0.125 to 0.125
- content_matrix: bfloat16 [2048, 2048], P(None, 'tp'), may hold values from -0.125 to 0.125
- result_valve_matrix: bfloat16 [2048, 2048], P(None, 'tp'), may hold values from -0.125 to 0.125
- fading_shift_vector: float32 [1024], P('tp'), may hold values from -1.5 to 20
- extra_fade_amount: float32 [8192, 16], P('ep', 'tp'), may hold values from -0.7 to 0
- starting_memory: float32 [1024, 128], P('tp'), may hold values from -24 to 24
- subspace_gain_vector: float32 [2048], P('tp'), may hold values from 0.1 to 1.9
- result_matrix: bfloat16 [2048, 2048], replicated, may hold values from -0.125 to 0.125
- specialist_microbatch: bfloat16 [4096, 2048], P(('ep', 'tp')), may hold values from -6 to 6
- specialist_gain_vector: float32 [2048], replicated, may hold values from 0.1 to 1.9
- picked_specialists: int32 [4096, 2], P(('ep', 'tp')), may hold values from 0 to 15, all different within a row; in each aligned block of 128 rows (0 to 127, 128 to 255, ...) at most 24 rows name the same one
- specialist_mixing_factor: float32 [4096, 2], P(('ep', 'tp')), may hold values from 0.3 to 1.5
- specialist_valve_matrix: bfloat16 [16, 2048, 1024], P('ep', None, 'tp'), may hold values from -0.125 to 0.125
- specialist_widen_matrix: bfloat16 [16, 2048, 1024], P('ep', None, 'tp'), may hold values from -0.125 to 0.125
- specialist_shrink_matrix: bfloat16 [16, 1024, 2048], P('ep', 'tp'), may hold values from -0.1875 to 0.1875
- joint_valve_matrix: bfloat16 [2048, 512], P(None, 'tp'), may hold values from -0.125 to 0.125
- joint_widen_matrix: bfloat16 [2048, 512], P(None, 'tp'), may hold values from -0.125 to 0.125
- joint_shrink_matrix: bfloat16 [512, 2048], P('tp'), may hold values from -0.25 to 0.25
Outputs:
- mixer_sublayer_result: bfloat16 [8192, 2048], P(('ep', 'tp'))
- moe_out: bfloat16 [4096, 2048], P(('ep', 'tp'))
The draws below stay inside these ranges and needn't reach their ends.
Inputs may be any that keep to these rules, and one draw needn't show every extreme that they name: `picked_specialists`: each row names 2 different experts; among the rows of one device no expert is named more than 24 times.
All inputs are finite; a program needn't handle non-finite values.
Results may differ from the reference program's by a relative error of at most 0.025.
Values may be sent and summed in bfloat16 or wider, within the bound.
No kernel may reach another device: no remote copies, remote signals or barrier semaphores. Data moves between devices by JAX's collectives and lax.ppermute only.
A program may use at most 192 MiB of HBM per device.

```python
import math
import jax
import jax.numpy as jnp
import numpy as np
from jax import lax

D = 2048
NUM_SUBSPACES = 16
MATCHER_WIDTH = 64
DV = 128
SPAN_LENGTH = 64
TOK_MOE = 128
TOP_K = 2
FFE = 1024
FFS = 512
EXPERTS = 16
CAP = 24
TOKENS_A = 8192
TOKENS_B = 4096
N_EP = 8
N_TP = 4


def draw_fading_shift_vector(key, part):
    key_one, key_two, key_three = jax.random.split(jax.random.fold_in(key, 11), 3)
    shuffled = jax.random.permutation(key_one, NUM_SUBSPACES)
    fast_head = shuffled < NUM_SUBSPACES // 2
    slow_value = jnp.log(jnp.float32(TOKENS_A) * 0.206)
    fast_value = jax.random.uniform(key_two, (NUM_SUBSPACES, MATCHER_WIDTH), jnp.float32, -1.0, 0.5)
    jitter = jax.random.uniform(key_three, (NUM_SUBSPACES, MATCHER_WIDTH), jnp.float32, -0.5, 0.5)
    result_value = jnp.where(fast_head[:, None], fast_value, slow_value + jitter)
    return result_value.reshape(NUM_SUBSPACES * MATCHER_WIDTH).astype(jnp.float32)


def draw_extra_fade_amount(key, part):
    key_one, key_two = jax.random.split(jax.random.fold_in(key, 23), 2)
    where_rows = jax.random.randint(key_one, (3,), 0, TOKENS_A)
    drop_depth = jnp.log(jax.random.uniform(key_two, (3, NUM_SUBSPACES), jnp.float32, 0.5, 0.8))
    positions = jnp.arange(TOKENS_A, dtype=jnp.int32)
    matches = (positions[:, None] == where_rows[None, :]).astype(jnp.float32)
    return jnp.dot(matches, drop_depth, precision=lax.Precision.HIGHEST)


def block_scale(rng, extent, cuts, least, largest):
    factor_of = 1.0
    for axis_at, parts in cuts:
        steps = jax.random.uniform(jax.random.fold_in(jax.random.fold_in(rng, 6), axis_at), (parts,), jnp.float32, least / len(cuts), largest / len(cuts))
        factor_of = factor_of * jnp.repeat(jnp.exp(steps), extent[axis_at] // parts).reshape((-1,) + (1,) * (len(extent) - 1 - axis_at))
    return factor_of


def shared_out(key, own, number, rows, amount, top, limit, slope):
    ranking = jax.random.permutation(key, amount)
    packed, ordinary = portions_of(amount, rows * top, limit, slope, True), portions_of(amount, rows * top, limit, slope, False)
    places = jnp.arange(amount)

    def named(sizes, offset_by):
        used = int((sizes > 0).sum())
        fixed = max(1, used // 4)
        moved = fixed + (places - fixed + offset_by * (used - fixed)) % max(1, amount - fixed)
        return jnp.zeros((amount,), jnp.int32).at[ranking[jnp.where(places < fixed, places, moved)]].set(jnp.asarray(sizes, jnp.int32))

    sizes = jnp.where(number % 4 == 0, named(packed, number // 4), named(ordinary, number - number // 4 - 1))
    mixed = jax.random.permutation(jax.random.fold_in(own, 3), amount)
    giver, receiver = mixed[0:amount // 2 * 2:2], mixed[1:amount // 2 * 2:2]
    margin = jnp.minimum(sizes[giver] - 1, limit - sizes[receiver]) // 2
    margin = jnp.where((giver == ranking[0]) | (receiver == ranking[0]) | (sizes[receiver] == 0), 0, jnp.maximum(margin, 0))
    moved = jax.random.randint(jax.random.fold_in(own, 4), (amount // 2,), 0, 1 << 20) % (margin + 1)
    sizes = sizes.at[giver].add(-moved).at[receiver].add(moved)
    members = jnp.searchsorted(jnp.cumsum(sizes), jnp.arange(rows * top), side="right").astype(jnp.int32)
    listing = members.reshape(top, rows).T
    listing = listing[jax.random.permutation(jax.random.fold_in(own, 1), rows)]
    offset_by = jax.random.randint(jax.random.fold_in(own, 2), (rows, 1), 0, top)
    return jnp.take_along_axis(listing, (jnp.arange(top)[None, :] + offset_by) % top, axis=1)


def portions_of(number_of, total, most, lean, full):
    portions = [(1 << 20) // math.isqrt(grade ** lean) + 1 for grade in range(1, number_of + 1)]
    largest = most if full else min(most, max(-(-total // number_of), total * portions[0] // sum(portions)))
    least = 1 if total - largest >= number_of - 1 else 0
    holding, spare = [largest] + [least] * (number_of - 1), total - largest - least * (number_of - 1)
    while spare > 0:
        free = [i for i in range(1, number_of) if holding[i] < largest] or [i for i in range(1, number_of) if holding[i] < most]
        mass, left = sum([portions[i] for i in free]), spare
        for i in free:
            more = min(most - holding[i], max(1, left * portions[i] // mass), spare)
            holding[i] = holding[i] + more
            spare = spare - more
    return np.array(holding)


def bell_draw(rng, dims, scale, limit, cuts=(), held_as=jnp.bfloat16):
    drawn = jax.random.normal(rng, dims, jnp.float32) * scale
    if len(cuts) > 0:
        drawn = block_scale(rng, dims, cuts, -0.22, 0.18) * drawn
    return jnp.clip(drawn, min=-limit, max=limit).astype(held_as)


def setup_inputs(seed: int = 0) -> dict:
    arg_keys = jax.random.split(jax.random.key(seed), 23)
    mixer_microbatch = bell_draw(arg_keys[0], (TOKENS_A, D), 1.0, 6.0, ((0, 32),))
    mixer_gain_vector = jnp.clip(1.0 + 0.18 * jax.random.normal(arg_keys[1], (D,), jnp.float32), 0.1, 1.9)
    asker_matrix = bell_draw(arg_keys[2], (D, NUM_SUBSPACES * MATCHER_WIDTH), D ** -0.5, 0.125, ((1, 4),))
    matcher_matrix = bell_draw(arg_keys[3], (D, NUM_SUBSPACES * MATCHER_WIDTH), D ** -0.5, 0.125, ((1, 4),))
    fading_matrix = bell_draw(arg_keys[4], (D, NUM_SUBSPACES * MATCHER_WIDTH), D ** -0.5, 0.125, ((1, 4),))
    content_matrix = bell_draw(arg_keys[5], (D, NUM_SUBSPACES * DV), D ** -0.5, 0.125, ((1, 4),))
    result_valve_matrix = bell_draw(arg_keys[6], (D, NUM_SUBSPACES * DV), D ** -0.5, 0.125, ((1, 4),))
    fading_shift_vector = draw_fading_shift_vector(jax.random.fold_in(arg_keys[22], 71), 0)
    extra_fade_amount = draw_extra_fade_amount(jax.random.fold_in(arg_keys[22], 71), 0)
    starting_memory = bell_draw(arg_keys[9], (NUM_SUBSPACES * MATCHER_WIDTH, DV), 4.0, 24.0, ((0, 4),), jnp.float32)
    subspace_gain_vector = jnp.clip(1.0 + 0.18 * jax.random.normal(arg_keys[10], (NUM_SUBSPACES * DV,), jnp.float32), 0.1, 1.9)
    result_matrix = bell_draw(arg_keys[11], (NUM_SUBSPACES * DV, D), (NUM_SUBSPACES * DV) ** -0.5, 0.125)
    specialist_microbatch = bell_draw(arg_keys[12], (TOKENS_B, D), 1.0, 6.0, ((0, 32),))
    specialist_gain_vector = jnp.clip(1.0 + 0.18 * jax.random.normal(arg_keys[13], (D,), jnp.float32), 0.1, 1.9)
    picked_specialists_keys = jax.random.split(jax.random.fold_in(arg_keys[14], 1), TOKENS_B // TOK_MOE)
    picked_specialists_turns = jax.random.permutation(jax.random.fold_in(arg_keys[14], 3), TOKENS_B // TOK_MOE)
    picked_specialists = jax.vmap(lambda own, number: shared_out(jax.random.fold_in(arg_keys[14], 2), own, number, TOK_MOE, EXPERTS, TOP_K, CAP, 1))(picked_specialists_keys, picked_specialists_turns).reshape((TOKENS_B, TOP_K))
    specialist_mixing_factor = jnp.clip(jnp.exp(math.log(1.5) - 1.60943787 * jax.random.uniform(arg_keys[15], (TOKENS_B, TOP_K), jnp.float32) ** block_scale(arg_keys[15], (TOKENS_B, TOP_K), ((0, 32),), -0.2, 0.2)), 0.3, 1.5)
    specialist_valve_matrix = bell_draw(arg_keys[16], (EXPERTS, D, FFE), D ** -0.5, 0.125, ((0, 8), (2, 4)))
    specialist_widen_matrix = bell_draw(arg_keys[17], (EXPERTS, D, FFE), D ** -0.5, 0.125, ((0, 8), (2, 4)))
    specialist_shrink_matrix = bell_draw(arg_keys[18], (EXPERTS, FFE, D), FFE ** -0.5, 0.1875, ((0, 8), (1, 4)))
    joint_valve_matrix = bell_draw(arg_keys[19], (D, FFS), D ** -0.5, 0.125, ((1, 4),))
    joint_widen_matrix = bell_draw(arg_keys[20], (D, FFS), D ** -0.5, 0.125, ((1, 4),))
    joint_shrink_matrix = bell_draw(arg_keys[21], (FFS, D), FFS ** -0.5, 0.25, ((0, 4),))
    return dict(mixer_microbatch=mixer_microbatch, mixer_gain_vector=mixer_gain_vector, asker_matrix=asker_matrix, matcher_matrix=matcher_matrix, fading_matrix=fading_matrix, content_matrix=content_matrix, result_valve_matrix=result_valve_matrix, fading_shift_vector=fading_shift_vector, extra_fade_amount=extra_fade_amount, starting_memory=starting_memory, subspace_gain_vector=subspace_gain_vector, result_matrix=result_matrix, specialist_microbatch=specialist_microbatch, specialist_gain_vector=specialist_gain_vector, picked_specialists=picked_specialists, specialist_mixing_factor=specialist_mixing_factor, specialist_valve_matrix=specialist_valve_matrix, specialist_widen_matrix=specialist_widen_matrix, specialist_shrink_matrix=specialist_shrink_matrix, joint_valve_matrix=joint_valve_matrix, joint_widen_matrix=joint_widen_matrix, joint_shrink_matrix=joint_shrink_matrix)


NORM_EPS = 1e-06
GATE_SOFTNESS = 16.0
exact_precision = lax.Precision.HIGHEST

def rms_rows(values, gain):
    widened = values.astype(jnp.float32)
    inverse_rms = lax.rsqrt(lax.optimization_barrier(jnp.mean(widened * widened, axis=-1, keepdims=True)) + NORM_EPS)
    return (widened * inverse_rms * gain).astype(jnp.bfloat16)

def expert_apply(rows_in, gate_w, up_w, down_w):
    gate_value = jnp.dot(rows_in, gate_w, preferred_element_type=jnp.float32)
    up_value = jnp.dot(rows_in, up_w, preferred_element_type=jnp.float32)
    hidden = (jax.nn.silu(gate_value) * up_value).astype(jnp.bfloat16)
    group_width = down_w.shape[0] // N_TP
    combined = jnp.zeros((rows_in.shape[0], down_w.shape[1]), jnp.float32)
    for group_index in range(N_TP):
        row_lower = group_index * group_width
        partial_sum = jnp.dot(hidden[:, row_lower:row_lower + group_width], down_w[row_lower:row_lower + group_width], preferred_element_type=jnp.float32)
        rounded = lax.optimization_barrier(partial_sum.astype(jnp.bfloat16))
        combined = combined + rounded.astype(jnp.float32)
    return combined.astype(jnp.bfloat16)

def mixer_share(mixer_microbatch, mixer_gain_vector, asker_matrix, matcher_matrix, fading_matrix, content_matrix, result_valve_matrix, fading_shift_vector, extra_fade_amount, starting_memory, subspace_gain_vector, result_matrix):
    normed = rms_rows(mixer_microbatch, mixer_gain_vector)

    def project(weight):
        return jnp.dot(normed, weight, preferred_element_type=jnp.float32).astype(jnp.bfloat16)
    query, key_rows, decay_logits, value, gate_pre = (project(asker_matrix), project(matcher_matrix), project(fading_matrix), project(content_matrix), project(result_valve_matrix))
    logarithmic_fading_speed = jax.nn.log_sigmoid(decay_logits.astype(jnp.float32) + fading_shift_vector) / GATE_SOFTNESS
    span_sequence = TOKENS_A // SPAN_LENGTH
    dimension_signature = (span_sequence, SPAN_LENGTH, NUM_SUBSPACES, MATCHER_WIDTH)
    query_wide = query.astype(jnp.float32).reshape(dimension_signature) * MATCHER_WIDTH ** (-0.5)
    key_wide = key_rows.astype(jnp.float32).reshape(dimension_signature)
    value_wide = value.astype(jnp.float32).reshape(span_sequence, SPAN_LENGTH, NUM_SUBSPACES, DV)
    speed_expanded = logarithmic_fading_speed.reshape(dimension_signature) + extra_fade_amount.reshape(span_sequence, SPAN_LENGTH, NUM_SUBSPACES, 1)
    causal_mask = jnp.tril(jnp.ones((SPAN_LENGTH, SPAN_LENGTH), bool))

    def step(carried_state, inputs):
        query_block, key_block, block_values, rate_block = inputs
        running = jnp.cumsum(rate_block, axis=0)
        block_total = running[-1:]
        query_faded = query_block * jnp.exp(running)
        k_decayed = key_block * jnp.exp(-running)
        key_until_finish = key_block * jnp.exp(block_total - running)
        scores = jnp.einsum('ihk,jhk->hij', query_faded, k_decayed, precision=exact_precision)
        scores = jnp.where(causal_mask[None], scores, 0.0)
        inner_part = jnp.einsum('hij,jhv->ihv', scores, block_values, precision=exact_precision)
        outer_contribution = jnp.einsum('wzr,zrg->wzg', query_faded, carried_state, precision=exact_precision)
        added_terms = jnp.einsum('aqe,aqf->qef', key_until_finish, block_values, precision=exact_precision)
        updated = jnp.exp(block_total[0])[..., None] * carried_state + added_terms
        return (updated, inner_part + outer_contribution)
    first_state = starting_memory.astype(jnp.float32).reshape(NUM_SUBSPACES, MATCHER_WIDTH, DV)
    _, attended = lax.scan(step, first_state, (query_wide, key_wide, value_wide, speed_expanded))
    attended = attended.reshape(TOKENS_A, NUM_SUBSPACES, DV)
    inverse_rms = lax.rsqrt(lax.optimization_barrier(jnp.mean(attended * attended, axis=-1, keepdims=True)) + NORM_EPS)
    normed_heads = (attended * inverse_rms).reshape(TOKENS_A, NUM_SUBSPACES * DV) * subspace_gain_vector
    headed = (normed_heads * jax.nn.silu(gate_pre.astype(jnp.float32))).astype(jnp.bfloat16)
    return jnp.dot(headed, result_matrix, preferred_element_type=jnp.float32).astype(jnp.bfloat16)

def expert_half(specialist_microbatch, specialist_gain_vector, picked_specialists, specialist_mixing_factor, specialist_valve_matrix, specialist_widen_matrix, specialist_shrink_matrix, joint_valve_matrix, joint_widen_matrix, joint_shrink_matrix):
    normed = rms_rows(specialist_microbatch, specialist_gain_vector)
    devices = N_EP * N_TP
    flat_expert = picked_specialists.reshape(devices, TOK_MOE * TOP_K)
    matches = (flat_expert[..., None] == jnp.arange(EXPERTS, dtype=jnp.int32)).astype(jnp.int32)
    slot_rank = lax.optimization_barrier(jnp.sum(jnp.cumsum(matches, axis=1) * matches, axis=2)) - 1
    device_ids = jnp.arange(devices, dtype=jnp.int32)[:, None]
    column = device_ids * CAP + slot_rank
    token_ids = device_ids * TOK_MOE + jnp.arange(TOK_MOE * TOP_K, dtype=jnp.int32)[None, :] // TOP_K
    slot_table = jnp.full((EXPERTS, devices * CAP), TOKENS_B, jnp.int32).at[flat_expert, column].set(token_ids)
    padded = jnp.concatenate([normed, jnp.zeros((1, normed.shape[1]), jnp.bfloat16)], axis=0)

    def one_expert(expert_index):
        picked_rows = padded[slot_table[expert_index]]
        return expert_apply(picked_rows, specialist_valve_matrix[expert_index], specialist_widen_matrix[expert_index], specialist_shrink_matrix[expert_index])
    outputs = lax.map(one_expert, jnp.arange(EXPERTS, dtype=jnp.int32))
    picked = outputs[flat_expert, column].reshape(TOKENS_B, TOP_K, normed.shape[1])
    shared = expert_apply(normed, joint_valve_matrix, joint_widen_matrix, joint_shrink_matrix)
    combined = shared.astype(jnp.float32) + lax.optimization_barrier(jnp.sum(specialist_mixing_factor[:, :, None] * picked.astype(jnp.float32), axis=1))
    return combined.astype(jnp.bfloat16)

def reference(mixer_microbatch, mixer_gain_vector, asker_matrix, matcher_matrix, fading_matrix, content_matrix, result_valve_matrix, fading_shift_vector, extra_fade_amount, starting_memory, subspace_gain_vector, result_matrix, specialist_microbatch, specialist_gain_vector, picked_specialists, specialist_mixing_factor, specialist_valve_matrix, specialist_widen_matrix, specialist_shrink_matrix, joint_valve_matrix, joint_widen_matrix, joint_shrink_matrix):
    mixer_sublayer_result = mixer_share(mixer_microbatch, mixer_gain_vector, asker_matrix, matcher_matrix, fading_matrix, content_matrix, result_valve_matrix, fading_shift_vector, extra_fade_amount, starting_memory, subspace_gain_vector, result_matrix)
    moe_out = expert_half(specialist_microbatch, specialist_gain_vector, picked_specialists, specialist_mixing_factor, specialist_valve_matrix, specialist_widen_matrix, specialist_shrink_matrix, joint_valve_matrix, joint_widen_matrix, joint_shrink_matrix)
    return (mixer_sublayer_result, moe_out)
```

```python
import jax
import jax.numpy as jnp
import numpy as np
from jax import lax
from jax.experimental import pallas as pl
from jax.experimental.pallas import tpu as pltpu
from jax.sharding import PartitionSpec as P

MATCHER_WIDTH = 64
DV = 128
SPAN_LENGTH = 64

NORM_EPS = 1e-06
GATE_SOFTNESS = 16.0
exact_precision = lax.Precision.HIGHEST
f32 = jnp.float32
bf16 = jnp.bfloat16


def params(**kw):
    return pltpu.CompilerParams(vmem_limit_bytes=48 * 1024 * 1024, **kw)


def cost(flops, nbytes):
    return pl.CostEstimate(flops=int(flops), bytes_accessed=int(nbytes), transcendentals=0)


def vmem(count):
    return [pl.BlockSpec(memory_space=pltpu.VMEM)] * count


def dot(a, b, dims=((1,), (0,))):
    return lax.dot_general(a, b, (dims, ((), ())), preferred_element_type=f32)


def rms_rows(values, gain):
    widened = values.astype(f32)
    inverse_rms = lax.rsqrt(jnp.mean(widened * widened, axis=-1, keepdims=True) + NORM_EPS)
    return (widened * inverse_rms * gain).astype(bf16)


def silu(v):
    return v * jax.nn.sigmoid(v)


def split_two(v):
    high = v.astype(bf16)
    return high, (v - high.astype(f32)).astype(bf16)


def split_three(v):
    high = v.astype(bf16)
    rest = v - high.astype(f32)
    mid = rest.astype(bf16)
    return high, mid, (rest - mid.astype(f32)).astype(bf16)


def permuted(x, axis, pairs):
    return lax.ppermute(x, axis, pairs)


def slot_choice(meta, slot_expert, slot_place, experts):
    tokens = meta.shape[0]
    top = meta.shape[1] // 2
    lane = lax.broadcasted_iota(jnp.int32, (tokens, experts), 1).astype(f32)
    named = jnp.zeros((tokens, experts), f32)
    weight = jnp.zeros((tokens, experts), f32)
    for k in range(top):
        hit = meta[:, k : k + 1] == lane
        named = named + jnp.where(hit, 1.0, 0.0)
        weight = weight + jnp.where(hit, meta[:, top + k : top + k + 1], 0.0)
    row = lax.broadcasted_iota(jnp.int32, (tokens, tokens), 0)
    column = lax.broadcasted_iota(jnp.int32, (tokens, tokens), 1)
    earlier = jnp.where(row > column, 1.0, 0.0).astype(bf16)
    rank = dot(earlier, named.astype(bf16))
    slots = slot_expert.shape[1]
    spread = (
        lax.broadcasted_iota(jnp.int32, (experts, slots), 0).astype(f32) == slot_expert
    )
    spread = jnp.where(spread, 1.0, 0.0).astype(bf16)
    named_at = dot(named.astype(bf16), spread)
    rank_at = dot(rank.astype(bf16), spread)
    w1, w2, w3 = split_three(weight)
    weight_at = dot(w1, spread) + dot(w2, spread) + dot(w3, spread)
    chosen = (named_at > 0.5) & (rank_at == slot_place)
    return chosen, jnp.where(chosen, weight_at, 0.0)


def pack_own_kernel(experts, x_ref, gain_ref, meta_ref, table_ref, normed_ref, out_ref, weight_ref):
    normed = rms_rows(x_ref[...], gain_ref[...])
    normed_ref[...] = normed
    chosen, weights = slot_choice(
        meta_ref[...], table_ref[0:1, :], table_ref[1:2, :], experts
    )
    pick = jnp.where(chosen, 1.0, 0.0).astype(bf16)
    out_ref[...] = dot(pick, normed, ((0,), (0,))).astype(bf16)
    weight_ref[...] = weights


def pack_both_kernel(
    experts, own_ref, x_ref, gain_ref, meta_ref, meta_x_ref, table_ref, tok_ref, out_ref, weight_ref
):
    tokens = own_ref.shape[0]
    table = table_ref[...]
    tok_ref[:tokens] = own_ref[...]
    tok_ref[tokens:] = rms_rows(x_ref[...], gain_ref[...])
    picks = []
    for index, ref in enumerate((meta_ref, meta_x_ref)):
        chosen, weights = slot_choice(ref[...], table[0:1, :], table[1:2, :], experts)
        mine = table[2:3, :] == float(index)
        weights = jnp.where(mine, weights, 0.0)
        weight_ref[index * tokens : (index + 1) * tokens, :] = weights
        picks.append(jnp.where(chosen & mine, 1.0, 0.0).astype(bf16))
    pick = jnp.concatenate(picks, axis=0)
    out_ref[...] = dot(pick, tok_ref[...], ((0,), (0,))).astype(bf16)


def ffn_kernel(arrays, peer_from, *refs):
    ins = refs[:arrays]
    gate_ref, up_ref, down_ref, mine_ref, peer_ref = refs[arrays:]
    rows = jnp.concatenate([r[...] for r in ins], axis=0)
    gate_w, up_w, down_w = gate_ref[...], up_ref[...], down_ref[...]
    if len(gate_w.shape) == 3:
        gate_w, up_w, down_w = gate_w[0], up_w[0], down_w[0]
    hidden = (silu(dot(rows, gate_w)) * dot(rows, up_w)).astype(bf16)
    result = dot(hidden, down_w).astype(bf16)
    height = ins[0].shape[0]
    for k in range(arrays):
        piece = result[k * height : (k + 1) * height]
        if k < peer_from:
            mine_ref[k] = piece
        else:
            peer_ref[k - peer_from] = piece


def ffn(rows, gate_w, up_w, down_w, expert, steps, name):
    arrays = len(rows)
    half = arrays // 2
    count, width = rows[0].shape
    height = count // steps
    row_spec = pl.BlockSpec((height, width), lambda i: (i, 0))
    if expert is None:
        weight_specs = [pl.BlockSpec(w.shape, lambda i: (0, 0)) for w in (gate_w, up_w, down_w)]
        inner = gate_w.shape[1]
    else:
        weight_specs = [
            pl.BlockSpec((1,) + w.shape[1:], lambda i: (expert, 0, 0))
            for w in (gate_w, up_w, down_w)
        ]
        inner = gate_w.shape[2]
    out = jax.ShapeDtypeStruct((half, count, width), bf16)
    out_spec = pl.BlockSpec((half, height, width), lambda i: (0, i, 0))
    return pl.pallas_call(
        lambda *refs: ffn_kernel(arrays, half, *refs),
        grid=(steps,),
        in_specs=[row_spec] * arrays + weight_specs,
        out_specs=[out_spec, out_spec],
        out_shape=[out, out],
        compiler_params=params(),
        cost_estimate=cost(
            6 * arrays * count * width * inner, 4 * arrays * count * width + 6 * width * inner
        ),
        name=name,
    )(*rows, gate_w, up_w, down_w)


def combine_kernel(ret_ref, weight_ref, mine_ref, got_ref, own_ref, send_ref):
    high, low = split_two(weight_ref[...])
    ret = ret_ref[...]
    total = dot(high, ret) + dot(low, ret)
    half = own_ref.shape[0]
    own_ref[...] = total[:half] + mine_ref[0].astype(f32) + got_ref[0].astype(f32)
    send_ref[...] = (total[half:] + mine_ref[1].astype(f32) + got_ref[1].astype(f32)).astype(bf16)


def finish_kernel(ret_ref, weight_ref, own_ref, got_ref, out_ref):
    high, low = split_two(weight_ref[...])
    ret = ret_ref[...]
    total = dot(high, ret) + dot(low, ret) + own_ref[...] + got_ref[...].astype(f32)
    out_ref[...] = total.astype(bf16)


def column_split(kernel, ins, blocked, outs, steps, flops, name):
    specs = []
    for a, cut in zip(ins, blocked):
        lead = a.shape[:-1]
        zeros = (0,) * len(lead)
        if cut:
            specs.append(pl.BlockSpec(lead + (a.shape[-1] // steps,), lambda i, z=zeros: z + (i,)))
        else:
            specs.append(pl.BlockSpec(a.shape, lambda i, z=zeros: z + (0,)))
    out_specs = [
        pl.BlockSpec(o.shape[:-1] + (o.shape[-1] // steps,), lambda i: (0, i)) for o in outs
    ]
    return pl.pallas_call(
        kernel,
        grid=(steps,),
        in_specs=specs,
        out_specs=out_specs,
        out_shape=outs,
        compiler_params=params(),
        cost_estimate=cost(flops, sum(a.size * a.dtype.itemsize for a in ins)),
        name=name,
    )(*ins)


def local_kernel(
    tp_count,
    heads,
    place_ref,
    *refs,
):
    raws = refs[:tp_count]
    (
        gain_ref,
        q_ref,
        k_ref,
        d_ref,
        v_ref,
        g_ref,
        shift_ref,
        fade_ref,
        out_ref,
        qg_ref,
        gate_ref,
        pack_ref,
        buffer,
        state,
        base,
        sems,
    ) = refs[tp_count:]
    step = pl.program_id(0)
    slot = jnp.bitwise_xor(step, place_ref[0])
    span = SPAN_LENGTH
    key_width = q_ref.shape[1]
    value_width = v_ref.shape[1]

    @pl.when(step == 0)
    def _():
        for n in range(tp_count):
            pltpu.make_async_copy(raws[n], buffer.at[n], sems.at[n]).start()
        state[...] = jnp.zeros_like(state)
        base[...] = jnp.zeros_like(base)

    pltpu.make_async_copy(raws[0], buffer.at[slot], sems.at[slot]).wait()
    normed = rms_rows(buffer[slot], gain_ref[...])
    rows = normed.shape[0]
    query = dot(normed, q_ref[...]).astype(bf16).astype(f32) * MATCHER_WIDTH ** (-0.5)
    keys = dot(normed, k_ref[...]).astype(bf16).astype(f32)
    logits = dot(normed, d_ref[...]).astype(bf16).astype(f32) + shift_ref[...]
    value = dot(normed, v_ref[...]).astype(bf16)
    gate_ref[...] = dot(normed, g_ref[...]).astype(bf16)

    head_row = lax.broadcasted_iota(jnp.int32, (heads, key_width), 0)
    head_lane = lax.broadcasted_iota(jnp.int32, (heads, key_width), 1)
    low = head_row * MATCHER_WIDTH
    spread = jnp.where((head_lane >= low) & (head_lane < low + MATCHER_WIDTH), 1.0, 0.0).astype(bf16)
    f1, f2, f3 = split_three(fade_ref[...])
    fade = dot(f1, spread) + dot(f2, spread) + dot(f3, spread)
    soft = jnp.minimum(logits, 0.0) - jnp.log1p(jnp.exp(-jnp.abs(logits)))
    rate = soft / GATE_SOFTNESS + fade

    row = lax.broadcasted_iota(jnp.int32, (rows, rows), 0)
    column = lax.broadcasted_iota(jnp.int32, (rows, rows), 1)
    span_bits = span.bit_length() - 1
    same_span = jnp.right_shift(row, span_bits) == jnp.right_shift(column, span_bits)
    lower = jnp.where(same_span & (row >= column), 1.0, 0.0).astype(bf16)
    r1, r2, r3 = split_three(rate)
    running = dot(lower, r1) + dot(lower, r2) + dot(lower, r3)
    query_faded = query * jnp.exp(running)
    key_decayed = (keys * jnp.exp(-running)).astype(bf16)

    width_bits = MATCHER_WIDTH.bit_length() - 1
    value_bits = DV.bit_length() - 1
    lane_head = jnp.right_shift(
        lax.broadcasted_iota(jnp.int32, (span, key_width), 1), width_bits
    )
    causal = (
        jnp.bitwise_and(lax.broadcasted_iota(jnp.int32, (heads * span, span), 0), span - 1)
        >= lax.broadcasted_iota(jnp.int32, (heads * span, span), 1)
    )
    own_block = jnp.right_shift(
        lax.broadcasted_iota(jnp.int32, (value_width, key_width), 0), value_bits
    ) == jnp.right_shift(lax.broadcasted_iota(jnp.int32, (value_width, key_width), 1), width_bits)

    held = state[...]
    passed = base[...]
    for n in range(rows // span):
        at = slice(n * span, (n + 1) * span)
        qf = query_faded[at]
        total = running[(n + 1) * span - 1 : (n + 1) * span]
        qb = qf.astype(bf16)
        vb = value[at]
        key_end = (keys[at] * jnp.exp(total - running[at])).astype(bf16)
        stacked = jnp.concatenate(
            [jnp.where(lane_head == h, qf, 0.0) for h in range(heads)], axis=0
        ).astype(bf16)
        scores = dot(stacked, key_decayed[at], ((1,), (1,)))
        scores = jnp.where(causal, scores, 0.0).astype(bf16)
        inner = jnp.concatenate(
            [
                dot(scores[h * span : (h + 1) * span], vb[:, h * DV : (h + 1) * DV])
                for h in range(heads)
            ],
            axis=1,
        )
        outer = dot(qb, held.astype(bf16), ((1,), (1,)))
        out_ref[at, :] = inner + outer
        qg_ref[at, :] = (qf * jnp.exp(passed)).astype(bf16)
        added = dot(vb, key_end, ((0,), (0,)))
        held = held * jnp.exp(total) + jnp.where(own_block, added, 0.0)
        passed = passed + total
    state[...] = held
    base[...] = passed

    @pl.when(step == pl.num_programs(0) - 1)
    def _():
        compact = held[0:DV]
        for h in range(1, heads):
            compact = compact + held[h * DV : (h + 1) * DV]
        pack_ref[0:DV, :] = compact.astype(bf16)
        pack_ref[DV:, :] = jnp.broadcast_to(
            jnp.exp(passed), (pack_ref.shape[0] - DV, key_width)
        ).astype(bf16)


def gated_kernel(
    heads, received, place_ref, local_ref, qg_ref, gate_ref, gain_ref, first_ref, *refs
):
    packs = refs[:received]
    out_ref, entering = refs[received:]
    key_width = qg_ref.shape[1]
    value_width = local_ref.shape[1]

    @pl.when(pl.program_id(0) == 0)
    def _():
        held = first_ref[...]
        for shift in range(received, 0, -1):
            got = packs[shift - 1]
            joined = held * got[DV : DV + 1, :].astype(f32) + got[0:DV, :].astype(f32)
            held = jnp.where(place_ref[0] >= shift, joined, held)
        width_bits = MATCHER_WIDTH.bit_length() - 1
        lane_head = jnp.right_shift(
            lax.broadcasted_iota(jnp.int32, (DV, key_width), 1), width_bits
        )
        for h in range(heads):
            entering[h * DV : (h + 1) * DV, :] = jnp.where(lane_head == h, held, 0.0).astype(bf16)

    attended = local_ref[...] + dot(qg_ref[...], entering[...], ((1,), (1,)))
    for h in range(heads):
        at = slice(h * DV, (h + 1) * DV)
        part = attended[:, at]
        inverse = lax.rsqrt(jnp.mean(part * part, axis=-1, keepdims=True) + NORM_EPS)
        out = part * inverse * gain_ref[:, at] * silu(gate_ref[:, at].astype(f32))
        out_ref[0, :, at] = out.astype(bf16)


def project_kernel(groups, x_ref, w_ref, out_ref):
    width = x_ref.shape[2]
    total = dot(x_ref[0], w_ref[0:width, :])
    for n in range(1, groups):
        total = total + dot(x_ref[n], w_ref[n * width : (n + 1) * width, :])
    out_ref[...] = total.astype(bf16)


def body(
    mixer_microbatch,
    mixer_gain_vector,
    asker_matrix,
    matcher_matrix,
    fading_matrix,
    content_matrix,
    result_valve_matrix,
    fading_shift_vector,
    extra_fade_amount,
    starting_memory,
    subspace_gain_vector,
    result_matrix,
    specialist_microbatch,
    specialist_gain_vector,
    picked_specialists,
    specialist_mixing_factor,
    specialist_valve_matrix,
    specialist_widen_matrix,
    specialist_shrink_matrix,
    joint_valve_matrix,
    joint_widen_matrix,
    joint_shrink_matrix,
):
    ep_count = lax.axis_size("ep")
    tp_count = lax.axis_size("tp")
    across = [(t, t ^ 2) for t in range(tp_count)]
    beside = [(t, t ^ 1) for t in range(tp_count)]
    ep_place = lax.axis_index("ep").astype(jnp.int32).reshape(1)
    tp_place = lax.axis_index("tp").astype(jnp.int32).reshape(1)

    tokens, feature_width = specialist_microbatch.shape
    top_count = picked_specialists.shape[1]
    local_experts = specialist_widen_matrix.shape[0]
    if local_experts != 2 or tp_count != 4:
        raise ValueError("unsupported sizes")
    experts = local_experts * ep_count
    slots = max(2, 3 * tokens * top_count // (2 * experts))

    meta = jnp.concatenate(
        [picked_specialists.astype(f32), specialist_mixing_factor], axis=1
    )
    meta_x = permuted(meta, "tp", across)
    moe_raw_x = permuted(specialist_microbatch, "tp", across)
    mix_raw_x = permuted(mixer_microbatch, "tp", across)
    mix_raw_c = permuted(mixer_microbatch, "tp", beside)
    mix_raw_xc = permuted(mix_raw_x, "tp", beside)

    near = ep_count * slots
    near_table = np.zeros((8, near), np.float32)
    c = np.arange(near)
    near_table[0] = (c // slots) * local_experts
    near_table[1] = c % slots
    far = 2 * near
    far_table = np.zeros((8, far), np.float32)
    c = np.arange(far)
    far_table[0] = (c // (2 * slots)) * local_experts + 1
    far_table[1] = c % slots
    far_table[2] = (c // slots) % 2

    moe_gain = specialist_gain_vector.reshape(1, -1)
    normed, near_out, near_weight = pl.pallas_call(
        lambda *r: pack_own_kernel(experts, *r),
        in_specs=vmem(4),
        out_specs=vmem(3),
        out_shape=[
            jax.ShapeDtypeStruct((tokens, feature_width), bf16),
            jax.ShapeDtypeStruct((near, feature_width), bf16),
            jax.ShapeDtypeStruct((tokens, near), f32),
        ],
        compiler_params=params(),
        cost_estimate=cost(2e9, 4e6),
        name="pack_own",
    )(specialist_microbatch, moe_gain, meta, jnp.asarray(near_table))

    def exchange(rows):
        shape = rows.shape
        cut = rows.reshape(ep_count, shape[0] // ep_count, shape[1])
        return lax.all_to_all(cut, "ep", split_axis=0, concat_axis=0, tiled=True).reshape(shape)

    near_in = exchange(near_out)

    toks, far_out, far_weight = pl.pallas_call(
        lambda *r: pack_both_kernel(experts, *r),
        in_specs=vmem(6),
        out_specs=vmem(3),
        out_shape=[
            jax.ShapeDtypeStruct((2 * tokens, feature_width), bf16),
            jax.ShapeDtypeStruct((far, feature_width), bf16),
            jax.ShapeDtypeStruct((2 * tokens, far), f32),
        ],
        compiler_params=params(),
        cost_estimate=cost(3e9, 6e6),
        name="pack_both",
    )(normed, moe_raw_x, moe_gain, meta, meta_x, jnp.asarray(far_table))
    far_in = exchange(far_out)
    toks_c = permuted(toks, "tp", beside)

    rows = mixer_microbatch.shape[0]
    key_width = asker_matrix.shape[1]
    value_width = content_matrix.shape[1]
    heads = value_width // DV
    sequence = rows * tp_count
    pack_rows = DV + 16
    whole = lambda a: pl.BlockSpec(a.shape, lambda i, *_: (0,) * len(a.shape))
    by_rows = lambda w: pl.BlockSpec((rows, w), lambda i, *_: (i, 0))
    mix_gain = mixer_gain_vector.reshape(1, -1)
    shift = fading_shift_vector.reshape(1, -1)
    weights = (asker_matrix, matcher_matrix, fading_matrix, content_matrix, result_valve_matrix)
    local, query_all, gate_pre, pack = pl.pallas_call(
        lambda *r: local_kernel(tp_count, heads, *r),
        grid_spec=pltpu.PrefetchScalarGridSpec(
            num_scalar_prefetch=1,
            grid=(tp_count,),
            in_specs=[pl.BlockSpec(memory_space=pl.ANY)] * tp_count
            + [whole(mix_gain)]
            + [whole(w) for w in weights]
            + [whole(shift), by_rows(heads)],
            out_specs=[
                by_rows(value_width),
                by_rows(key_width),
                by_rows(value_width),
                pl.BlockSpec((pack_rows, key_width), lambda i, *_: (0, 0)),
            ],
            scratch_shapes=[
                pltpu.VMEM((tp_count, rows, feature_width), bf16),
                pltpu.VMEM((value_width, key_width), f32),
                pltpu.VMEM((1, key_width), f32),
                pltpu.SemaphoreType.DMA((tp_count,)),
            ],
        ),
        out_shape=[
            jax.ShapeDtypeStruct((sequence, value_width), f32),
            jax.ShapeDtypeStruct((sequence, key_width), bf16),
            jax.ShapeDtypeStruct((sequence, value_width), bf16),
            jax.ShapeDtypeStruct((pack_rows, key_width), bf16),
        ],
        compiler_params=params(),
        cost_estimate=cost(2e10, 2e7),
        name="local_attention",
    )(
        tp_place,
        mixer_microbatch,
        mix_raw_c,
        mix_raw_x,
        mix_raw_xc,
        mix_gain,
        *weights,
        shift,
        extra_fade_amount,
    )
    packs = [
        permuted(pack, "ep", [(e, e + s) for e in range(ep_count - s)])
        for s in range(1, ep_count)
    ]
    first = starting_memory.T
    head_gain = subspace_gain_vector.reshape(1, -1)
    gated = pl.pallas_call(
        lambda *r: gated_kernel(heads, ep_count - 1, *r),
        grid_spec=pltpu.PrefetchScalarGridSpec(
            num_scalar_prefetch=1,
            grid=(tp_count,),
            in_specs=[by_rows(value_width), by_rows(key_width), by_rows(value_width)]
            + [whole(head_gain), whole(first)]
            + [whole(pack)] * (ep_count - 1),
            out_specs=pl.BlockSpec((1, rows, value_width), lambda i, *_: (i, 0, 0)),
            scratch_shapes=[pltpu.VMEM((value_width, key_width), bf16)],
        ),
        out_shape=jax.ShapeDtypeStruct((tp_count, rows, value_width), bf16),
        compiler_params=params(),
        cost_estimate=cost(2e9, 6e6),
        name="gated_heads",
    )(ep_place, local, query_all, gate_pre, head_gain, first, *packs)
    per_token = lax.all_to_all(gated, "tp", split_axis=0, concat_axis=0, tiled=True)

    near_x = permuted(near_in, "tp", across)
    near_c = permuted(near_in, "tp", beside)
    near_xc = permuted(near_x, "tp", beside)
    far_c = permuted(far_in, "tp", beside)
    shared_mine, shared_peer = ffn(
        [toks[:tokens], toks[tokens:], toks_c[:tokens], toks_c[tokens:]],
        joint_valve_matrix,
        joint_widen_matrix,
        joint_shrink_matrix,
        None,
        1,
        "shared_ffn",
    )
    shared_got = permuted(shared_peer, "tp", beside)
    expert_weights = (specialist_valve_matrix, specialist_widen_matrix, specialist_shrink_matrix)
    near_mine, near_peer = ffn(
        [near_in, near_x, near_c, near_xc], *expert_weights, 0, 2, "near_ffn"
    )
    near_got = permuted(near_peer, "tp", beside)
    near_send = (near_mine[1].astype(f32) + near_got[1].astype(f32)).astype(bf16)
    near_back = permuted(near_send, "tp", across)
    near_sum = (
        near_mine[0].astype(f32) + near_got[0].astype(f32) + near_back.astype(f32)
    ).astype(bf16)
    near_ret = exchange(near_sum)
    far_mine, far_peer = ffn([far_in, far_c], *expert_weights, 1, 2, "far_ffn")
    far_got = permuted(far_peer, "tp", beside)
    far_sum = (far_mine[0].astype(f32) + far_got[0].astype(f32)).astype(bf16)
    far_ret = exchange(far_sum)

    own, send = column_split(
        combine_kernel,
        (far_ret, far_weight, shared_mine, shared_got),
        (True, False, True, True),
        [
            jax.ShapeDtypeStruct((tokens, feature_width), f32),
            jax.ShapeDtypeStruct((tokens, feature_width), bf16),
        ],
        2,
        4 * 2 * tokens * far * feature_width,
        "combine_far",
    )
    send_x = permuted(send, "tp", across)
    (moe_out,) = column_split(
        finish_kernel,
        (near_ret, near_weight, own, send_x),
        (True, False, True, True),
        [jax.ShapeDtypeStruct((tokens, feature_width), bf16)],
        2,
        4 * tokens * near * feature_width,
        "finish",
    )

    columns = 4
    out_width = result_matrix.shape[1]
    mixer_sublayer_result = pl.pallas_call(
        lambda *r: project_kernel(tp_count, *r),
        grid=(columns,),
        in_specs=[
            pl.BlockSpec(per_token.shape, lambda i: (0, 0, 0)),
            pl.BlockSpec((result_matrix.shape[0], out_width // columns), lambda i: (0, i)),
        ],
        out_specs=pl.BlockSpec((rows, out_width // columns), lambda i: (0, i)),
        out_shape=jax.ShapeDtypeStruct((rows, out_width), bf16),
        compiler_params=params(),
        cost_estimate=cost(2 * rows * out_width * result_matrix.shape[0], 1e7),
        name="result_project",
    )(per_token, result_matrix)
    return (mixer_sublayer_result, moe_out)


def solution(mesh):
    return jax.shard_map(
        body,
        mesh=mesh,
        in_specs=(
            P(("ep", "tp"), None),
            P(),
            P(None, "tp"),
            P(None, "tp"),
            P(None, "tp"),
            P(None, "tp"),
            P(None, "tp"),
            P("tp"),
            P("ep", "tp"),
            P("tp", None),
            P("tp"),
            P(),
            P(("ep", "tp"), None),
            P(),
            P(("ep", "tp"), None),
            P(("ep", "tp"), None),
            P("ep", None, "tp"),
            P("ep", None, "tp"),
            P("ep", "tp", None),
            P(None, "tp"),
            P(None, "tp"),
            P("tp", None),
        ),
        out_specs=(P(("ep", "tp"), None), P(("ep", "tp"), None)),
        check_vma=False,
    )
```

```python
import jax
import jax.numpy as jnp
from jax import lax
from jax.experimental import pallas as pl
from jax.experimental.pallas import tpu as pltpu
from jax.sharding import PartitionSpec as P

MATCHER_WIDTH = 64
DV = 128
SPAN_LENGTH = 64

NORM_EPS = 1e-06
GATE_SOFTNESS = 16.0
f32 = jnp.float32
bf16 = jnp.bfloat16


def params(**kw):
    return pltpu.CompilerParams(**kw)


def cost(flops, nbytes):
    return pl.CostEstimate(flops=int(flops), bytes_accessed=int(nbytes), transcendentals=0)


def vmem(count):
    return [pl.BlockSpec(memory_space=pltpu.VMEM)] * count


def dot(a, b, dims=((1,), (0,))):
    return lax.dot_general(a, b, (dims, ((), ())), preferred_element_type=f32)


def rms_rows(values, gain):
    widened = values.astype(f32)
    inverse_rms = lax.rsqrt(jnp.mean(widened * widened, axis=-1, keepdims=True) + NORM_EPS)
    return (widened * inverse_rms * gain).astype(bf16)


def silu(v):
    return v * jax.nn.sigmoid(v)


def split_two(v):
    high = v.astype(bf16)
    return high, (v - high.astype(f32)).astype(bf16)


def split_three(v):
    high = v.astype(bf16)
    rest = v - high.astype(f32)
    mid = rest.astype(bf16)
    return high, mid, (rest - mid.astype(f32)).astype(bf16)


def slot_choice(picks, factors, slot_expert, slot_place, experts):
    top, tokens = picks.shape
    slots = slot_expert.shape[0]
    index = lax.broadcasted_iota(jnp.int32, (experts, tokens), 0).astype(f32)
    named = jnp.zeros((experts, tokens), f32)
    weight = jnp.zeros((experts, tokens), f32)
    for k in range(top):
        hit = picks[k : k + 1, :] == index
        named = named + jnp.where(hit, 1.0, 0.0)
        weight = weight + jnp.where(hit, factors[k : k + 1, :], 0.0)
    row = lax.broadcasted_iota(jnp.int32, (tokens, tokens), 0)
    column = lax.broadcasted_iota(jnp.int32, (tokens, tokens), 1)
    earlier = jnp.where(row < column, 1.0, 0.0).astype(bf16)
    rank = dot(named.astype(bf16), earlier)
    spread = lax.broadcasted_iota(jnp.int32, (slots, experts), 1).astype(f32) == slot_expert
    spread = jnp.where(spread, 1.0, 0.0).astype(bf16)
    named_at = dot(spread, named.astype(bf16))
    rank_at = dot(spread, rank.astype(bf16))
    w1, w2, w3 = split_three(weight)
    weight_at = dot(spread, w1) + dot(spread, w2) + dot(spread, w3)
    chosen = (named_at > 0.5) & (rank_at == slot_place)
    return jnp.where(chosen, 1.0, 0.0).astype(bf16), jnp.where(chosen, weight_at, 0.0)


def pack_own_kernel(experts, slots, place_ref, x_ref, gain_ref, picks_ref, factor_ref, *refs):
    normed_ref, weight_ref = refs[:2]
    outs = refs[2:]
    normed = rms_rows(x_ref[...], gain_ref[...])
    normed_ref[...] = normed
    row = lax.broadcasted_iota(jnp.int32, (weight_ref.shape[0], 1), 0)
    block = jnp.zeros(row.shape, jnp.int32)
    for n in range(1, len(outs)):
        block = block + jnp.where(row >= n * slots, 1, 0)
    owner = jnp.bitwise_xor(block, place_ref[0])
    local = experts // len(outs)
    pick, weights = slot_choice(
        picks_ref[...].astype(f32),
        factor_ref[...],
        (owner * local).astype(f32),
        (row - block * slots).astype(f32),
        experts,
    )
    rows = dot(pick, normed).astype(bf16)
    for n, ref in enumerate(outs):
        ref[...] = rows[n * slots : (n + 1) * slots]
    weight_ref[...] = weights


def pack_both_kernel(
    experts,
    slots,
    groups,
    own_ref,
    x_ref,
    gain_ref,
    picks_ref,
    factor_ref,
    picks_x_ref,
    factor_x_ref,
    tok_ref,
    out_ref,
    weight_ref,
):
    tok_ref[...] = rms_rows(x_ref[...], gain_ref[...])
    row = lax.broadcasted_iota(jnp.int32, (weight_ref.shape[0], 1), 0)
    block = jnp.zeros(row.shape, jnp.int32)
    for n in range(1, groups):
        block = block + jnp.where(row >= n * slots, 1, 0)
    local = experts // groups
    tables = ((block * local + 1).astype(f32), (row - block * slots).astype(f32))
    own, weights = slot_choice(picks_ref[...].astype(f32), factor_ref[...], *tables, experts)
    other, _ = slot_choice(picks_x_ref[...].astype(f32), factor_x_ref[...], *tables, experts)
    weight_ref[...] = weights
    rows = (dot(own, own_ref[...]).astype(bf16), dot(other, tok_ref[...]).astype(bf16))
    for n in range(groups):
        for k in range(2):
            out_ref[(2 * n + k) * slots : (2 * n + k + 1) * slots] = rows[k][
                n * slots : (n + 1) * slots
            ]


def ffn_kernel(arrays, slots, *refs):
    ins = refs[:arrays]
    weights = refs[arrays : arrays + 6]
    outs = refs[arrays + 6 :]
    rows = jnp.concatenate([r[...] for r in ins], axis=0)
    total = None
    for n in range(2):
        gate_w, up_w, down_w = (w[...] for w in weights[3 * n : 3 * n + 3])
        if len(gate_w.shape) == 3:
            gate_w, up_w, down_w = gate_w[0], up_w[0], down_w[0]
        hidden = (silu(dot(rows, gate_w)) * dot(rows, up_w)).astype(bf16)
        part = dot(hidden, down_w)
        total = part if total is None else total + part
    height = ins[0].shape[0]
    if len(outs) == arrays:
        for k in range(arrays):
            outs[k][...] = total[k * height : (k + 1) * height].astype(bf16)
        return
    for n in range(height // (2 * slots)):
        for k in range(2):
            piece = total[(2 * n + k) * slots : (2 * n + k + 1) * slots].astype(bf16)
            outs[k][n * slots : (n + 1) * slots] = piece


def ffn(rows, weights, expert, steps, slots=None):
    arrays = len(rows)
    count, width = rows[0].shape
    height = count // steps
    row_spec = pl.BlockSpec((height, width), lambda i: (i, 0))
    if expert is None:
        weight_specs = [pl.BlockSpec(w.shape, lambda i: (0, 0)) for w in weights]
        inner = 2 * weights[0].shape[1]
    else:
        weight_specs = [
            pl.BlockSpec((1,) + w.shape[1:], lambda i: (expert, 0, 0)) for w in weights
        ]
        inner = 2 * weights[0].shape[2]
    if slots is None:
        outs, parts = arrays, 1
    else:
        outs, parts = 2, 2
    out = jax.ShapeDtypeStruct((count // parts, width), bf16)
    return pl.pallas_call(
        lambda *refs: ffn_kernel(arrays, slots, *refs),
        grid=(steps,),
        in_specs=[row_spec] * arrays + weight_specs,
        out_specs=[pl.BlockSpec((height // parts, width), lambda i: (i, 0))] * outs,
        out_shape=[out] * outs,
        compiler_params=params(),
        cost_estimate=cost(
            6 * arrays * count * width * inner, 4 * arrays * count * width + 6 * width * inner
        ),
    )(*rows, *weights)


def join_kernel(*refs):
    height = refs[0].shape[0]
    for n, ref in enumerate(refs[:-1]):
        refs[-1][n * height : (n + 1) * height, :] = ref[...]


def sum_kernel(a_ref, b_ref, *outs):
    total = (a_ref[...].astype(f32) + b_ref[...].astype(f32)).astype(bf16)
    height = outs[0].shape[0]
    for n, ref in enumerate(outs):
        ref[...] = total[n * height : (n + 1) * height]


def finish_kernel(near_weight_ref, far_weight_ref, shared_ref, got_ref, far_ref, *refs):
    out_ref = refs[-1]
    total = shared_ref[...].astype(f32) + got_ref[...].astype(f32)
    near = jnp.concatenate([r[...] for r in refs[:-1]], axis=0)
    for weight_ref, ret in ((near_weight_ref, near), (far_weight_ref, far_ref[...])):
        for part in split_two(weight_ref[...]):
            total = total + dot(part, ret, ((0,), (0,)))
    out_ref[...] = total.astype(bf16)


def column_split(kernel, ins, blocked, outs, steps, flops):
    specs = []
    for a, cut in zip(ins, blocked):
        lead = a.shape[:-1]
        zeros = (0,) * len(lead)
        if cut:
            specs.append(pl.BlockSpec(lead + (a.shape[-1] // steps,), lambda i, z=zeros: z + (i,)))
        else:
            specs.append(pl.BlockSpec(a.shape, lambda i, z=zeros: z + (0,)))
    out_specs = [
        pl.BlockSpec(o.shape[:-1] + (o.shape[-1] // steps,), lambda i: (0, i)) for o in outs
    ]
    return pl.pallas_call(
        kernel,
        grid=(steps,),
        in_specs=specs,
        out_specs=out_specs,
        out_shape=outs,
        compiler_params=params(),
        cost_estimate=cost(flops, sum(a.size * a.dtype.itemsize for a in ins)),
    )(*ins)


def local_kernel(heads, place_ref, first_ref, second_ref, *refs):
    (
        gain_ref,
        q_ref,
        k_ref,
        d_ref,
        v_ref,
        g_ref,
        shift_ref,
        fade_ref,
        out_ref,
        qg_ref,
        gate_ref,
        pack_ref,
        buffer,
        sems,
    ) = refs
    slot = pl.program_id(0)
    span = SPAN_LENGTH
    key_width = q_ref.shape[1]
    value_width = v_ref.shape[1]

    @pl.when(slot == 0)
    def _():
        for n, ref in enumerate((first_ref, second_ref)):
            pltpu.make_async_copy(ref, buffer.at[n], sems.at[n]).start()

    pltpu.make_async_copy(first_ref, buffer.at[slot], sems.at[slot]).wait()
    normed = rms_rows(buffer[slot], gain_ref[...])
    rows = normed.shape[0]
    query = dot(normed, q_ref[...]).astype(bf16).astype(f32) * MATCHER_WIDTH ** (-0.5)
    keys = dot(normed, k_ref[...]).astype(bf16).astype(f32)
    logits = dot(normed, d_ref[...]).astype(bf16).astype(f32) + shift_ref[...]
    value = dot(normed, v_ref[...]).astype(bf16)
    gate_ref[0] = dot(normed, g_ref[...]).astype(bf16)

    head_row = lax.broadcasted_iota(jnp.int32, (heads, key_width), 0)
    head_lane = lax.broadcasted_iota(jnp.int32, (heads, key_width), 1)
    low = head_row * MATCHER_WIDTH
    spread = jnp.where((head_lane >= low) & (head_lane < low + MATCHER_WIDTH), 1.0, 0.0).astype(bf16)
    f1, f2, f3 = split_three(fade_ref[...])
    fade = dot(f1, spread) + dot(f2, spread) + dot(f3, spread)
    soft = jnp.minimum(logits, 0.0) - jnp.log1p(jnp.exp(-jnp.abs(logits)))
    rate = soft / GATE_SOFTNESS + fade

    row = lax.broadcasted_iota(jnp.int32, (rows, rows), 0)
    column = lax.broadcasted_iota(jnp.int32, (rows, rows), 1)
    span_bits = span.bit_length() - 1
    same_span = jnp.right_shift(row, span_bits) == jnp.right_shift(column, span_bits)
    lower = jnp.where(same_span & (row >= column), 1.0, 0.0).astype(bf16)
    r1, r2, r3 = split_three(rate)
    running = dot(lower, r1) + dot(lower, r2) + dot(lower, r3)
    query_faded = query * jnp.exp(running)
    key_decayed = (keys * jnp.exp(-running)).astype(bf16)

    width_bits = MATCHER_WIDTH.bit_length() - 1
    value_bits = DV.bit_length() - 1
    lane_head = jnp.right_shift(
        lax.broadcasted_iota(jnp.int32, (span, key_width), 1), width_bits
    )
    causal = (
        jnp.bitwise_and(lax.broadcasted_iota(jnp.int32, (heads * span, span), 0), span - 1)
        >= lax.broadcasted_iota(jnp.int32, (heads * span, span), 1)
    )
    own_block = jnp.right_shift(
        lax.broadcasted_iota(jnp.int32, (value_width, key_width), 0), value_bits
    ) == jnp.right_shift(lax.broadcasted_iota(jnp.int32, (value_width, key_width), 1), width_bits)

    held = jnp.zeros((value_width, key_width), f32)
    passed = jnp.zeros((1, key_width), f32)
    for n in range(rows // span):
        at = slice(n * span, (n + 1) * span)
        qf = query_faded[at]
        total = running[(n + 1) * span - 1 : (n + 1) * span]
        qb = qf.astype(bf16)
        vb = value[at]
        key_end = (keys[at] * jnp.exp(total - running[at])).astype(bf16)
        stacked = jnp.concatenate(
            [jnp.where(lane_head == h, qf, 0.0) for h in range(heads)], axis=0
        ).astype(bf16)
        scores = dot(stacked, key_decayed[at], ((1,), (1,)))
        scores = jnp.where(causal, scores, 0.0).astype(bf16)
        inner = jnp.concatenate(
            [
                dot(scores[h * span : (h + 1) * span], vb[:, h * DV : (h + 1) * DV])
                for h in range(heads)
            ],
            axis=1,
        )
        outer = dot(qb, held.astype(bf16), ((1,), (1,)))
        out_ref[0, at, :] = inner + outer
        qg_ref[0, at, :] = (qf * jnp.exp(passed)).astype(bf16)
        added = dot(vb, key_end, ((0,), (0,)))
        held = held * jnp.exp(total) + jnp.where(own_block, added, 0.0)
        passed = passed + total
    compact = held[0:DV]
    for h in range(1, heads):
        compact = compact + held[h * DV : (h + 1) * DV]
    pack_ref[0, 0:DV, :] = compact
    pack_ref[0, DV:, :] = jnp.broadcast_to(
        jnp.exp(passed), (pack_ref.shape[1] - DV, key_width)
    )


def follow(held, pack):
    return held * pack[DV : DV + 1].astype(f32) + pack[0:DV].astype(f32)


def store_pack(ref, held, fading):
    ref[0:DV, :] = held.astype(bf16)
    ref[DV:, :] = jnp.broadcast_to(fading, (ref.shape[0] - DV, fading.shape[1])).astype(bf16)


def block_pack(packs, slot):
    inner = jnp.bitwise_and(slot, 1)
    return jnp.where(slot >= 2, packs[1][inner], packs[0][inner])


def chain_kernel(blocks, place_ref, first_ref, second_ref, out_ref):
    held = None
    for n in range(blocks):
        pack = block_pack((first_ref, second_ref), jnp.bitwise_xor(place_ref[1], n))
        if held is None:
            held, fading = pack[0:DV], pack[DV : DV + 1]
        else:
            held, fading = follow(held, pack), fading * pack[DV : DV + 1]
    store_pack(out_ref, held, fading)


def pair_kernel(place_ref, own_ref, got_ref, out_ref):
    own, got = own_ref[...].astype(f32), got_ref[...].astype(f32)
    odd = jnp.bitwise_and(place_ref[0], 1) == 1
    earlier, later = jnp.where(odd, got, own), jnp.where(odd, own, got)
    store_pack(
        out_ref, follow(earlier[0:DV], later), earlier[DV : DV + 1] * later[DV : DV + 1]
    )


def gated_kernel(
    heads,
    blocks,
    first_slot,
    place_ref,
    local_ref,
    qg_ref,
    gate_ref,
    gain_ref,
    start_ref,
    pack_a_ref,
    pack_b_ref,
    even_ref,
    *refs,
):
    outs = refs[-3:-1]
    packs = refs[:-3]
    entering = refs[-1]
    key_width = qg_ref.shape[2]

    @pl.when(pl.program_id(0) == 0)
    def _():
        held = start_ref[...]
        pair = jnp.right_shift(place_ref[0], 1)
        for shift in range(len(packs), 0, -1):
            held = jnp.where(pair >= shift, follow(held, packs[shift - 1][...]), held)
        odd = jnp.bitwise_and(place_ref[0], 1) == 1
        held = jnp.where(odd, follow(held, even_ref[...]), held)
        width_bits = MATCHER_WIDTH.bit_length() - 1
        lane_head = jnp.right_shift(
            lax.broadcasted_iota(jnp.int32, (DV, key_width), 1), width_bits
        )
        for n in range(blocks):
            slot = jnp.bitwise_xor(place_ref[1], n)
            for h in range(heads):
                entering[slot, h * DV : (h + 1) * DV, :] = jnp.where(
                    lane_head == h, held, 0.0
                ).astype(bf16)
            held = follow(held, block_pack((pack_a_ref, pack_b_ref), slot))

    slot = pl.program_id(0) + first_slot
    attended = local_ref[0] + dot(qg_ref[0], entering[slot], ((1,), (1,)))
    parts = []
    for h in range(heads):
        at = slice(h * DV, (h + 1) * DV)
        part = attended[:, at]
        inverse = lax.rsqrt(jnp.mean(part * part, axis=-1, keepdims=True) + NORM_EPS)
        part = part * inverse * gain_ref[:, at] * silu(gate_ref[0, :, at].astype(f32))
        parts.append(part.astype(bf16))
    rows = jnp.concatenate(parts, axis=1)
    for n, ref in enumerate(outs):

        @pl.when(pl.program_id(0) == n)
        def _(ref=ref):
            ref[...] = rows


def project_kernel(groups, place_ref, *refs):
    w_ref, out_ref = refs[groups:]
    width = refs[0].shape[1]
    total = None
    for n in range(groups):
        first = pl.multiple_of(jnp.bitwise_xor(place_ref[0], n) * width, width)
        part = dot(refs[n][...], w_ref[pl.ds(first, width), :])
        total = part if total is None else total + part
    out_ref[...] = total.astype(bf16)


def body(
    mixer_microbatch,
    mixer_gain_vector,
    asker_matrix,
    matcher_matrix,
    fading_matrix,
    content_matrix,
    result_valve_matrix,
    fading_shift_vector,
    extra_fade_amount,
    starting_memory,
    subspace_gain_vector,
    result_matrix,
    specialist_microbatch,
    specialist_gain_vector,
    picked_specialists,
    specialist_mixing_factor,
    specialist_valve_matrix,
    specialist_widen_matrix,
    specialist_shrink_matrix,
    joint_valve_matrix,
    joint_widen_matrix,
    joint_shrink_matrix,
):
    ep_count = lax.axis_size("ep")
    tp_count = lax.axis_size("tp")
    across = [(t, t ^ 2) for t in range(tp_count)]
    beside = [(t, t ^ 1) for t in range(tp_count)]
    ep_place = lax.axis_index("ep").astype(jnp.int32).reshape(1)
    tp_place = lax.axis_index("tp").astype(jnp.int32).reshape(1)

    tokens, feature_width = specialist_microbatch.shape
    top_count = picked_specialists.shape[1]
    local_experts = specialist_widen_matrix.shape[0]
    if local_experts != 2 or tp_count != 4:
        raise ValueError("unsupported sizes")
    experts = local_experts * ep_count
    slots = max(2, 3 * tokens * top_count // (2 * experts))

    picks, factors = picked_specialists.T, specialist_mixing_factor.T
    moe_raw_x = lax.ppermute(specialist_microbatch, "tp", across)
    picks_x = lax.ppermute(picks, "tp", across)
    factors_x = lax.ppermute(factors, "tp", across)
    mix_raw_x = lax.ppermute(mixer_microbatch, "tp", across)
    mix_raw_c = lax.ppermute(mixer_microbatch, "tp", beside)
    mix_raw_xc = lax.ppermute(mix_raw_x, "tp", beside)
    joint_weights = (joint_valve_matrix, joint_widen_matrix, joint_shrink_matrix)
    joint_weights += tuple(lax.ppermute(w, "tp", beside) for w in joint_weights)
    expert_weights = (specialist_valve_matrix, specialist_widen_matrix, specialist_shrink_matrix)
    expert_weights += tuple(lax.ppermute(w, "tp", beside) for w in expert_weights)

    near = ep_count * slots
    far = 2 * near
    moe_gain = specialist_gain_vector.reshape(1, -1)
    piece = jax.ShapeDtypeStruct((slots, feature_width), bf16)
    smem = [pl.BlockSpec(memory_space=pltpu.SMEM)]
    normed, near_weight, *near_out = pl.pallas_call(
        lambda *r: pack_own_kernel(experts, slots, *r),
        in_specs=smem + vmem(4),
        out_specs=vmem(2 + ep_count),
        out_shape=[
            jax.ShapeDtypeStruct((tokens, feature_width), bf16),
            jax.ShapeDtypeStruct((near, tokens), f32),
        ]
        + [piece] * ep_count,
        compiler_params=params(),
        cost_estimate=cost(2e9, 4e6),
        name="pack_own",
    )(ep_place, specialist_microbatch, moe_gain, picks, factors)

    def swap(pieces):
        return [pieces[0]] + [
            lax.ppermute(pieces[n], "ep", [(e, e ^ n) for e in range(ep_count)])
            for n in range(1, ep_count)
        ]

    def exchange(rows):
        shape = rows.shape
        cut = rows.reshape(ep_count, shape[0] // ep_count, shape[1])
        out = lax.all_to_all(cut, "ep", split_axis=0, concat_axis=0, tiled=True)
        return out.reshape(shape)

    near_in = pl.pallas_call(
        join_kernel,
        in_specs=vmem(ep_count),
        out_specs=pl.BlockSpec(memory_space=pltpu.VMEM),
        out_shape=jax.ShapeDtypeStruct((near, feature_width), bf16),
        compiler_params=params(),
        cost_estimate=cost(1e9, 2e6),
        name="near_join",
    )(*swap(near_out))

    normed_x, far_out, far_weight = pl.pallas_call(
        lambda *r: pack_both_kernel(experts, slots, ep_count, *r),
        in_specs=vmem(7),
        out_specs=vmem(3),
        out_shape=[
            jax.ShapeDtypeStruct((tokens, feature_width), bf16),
            jax.ShapeDtypeStruct((far, feature_width), bf16),
            jax.ShapeDtypeStruct((near, tokens), f32),
        ],
        compiler_params=params(),
        cost_estimate=cost(3e9, 6e6),
        name="pack_both",
    )(
        normed,
        moe_raw_x,
        moe_gain,
        picks,
        factors,
        picks_x,
        factors_x,
    )
    far_in = exchange(far_out)

    rows = mixer_microbatch.shape[0]
    key_width = asker_matrix.shape[1]
    value_width = content_matrix.shape[1]
    heads = value_width // DV
    pack_rows = DV + 16
    place = jnp.concatenate([ep_place, tp_place])
    whole = lambda a: pl.BlockSpec(a.shape, lambda i, *_: (0,) * len(a.shape))
    by_slot = lambda r, w: pl.BlockSpec((1, r, w), lambda i, *_: (i, 0, 0))
    mix_gain = mixer_gain_vector.reshape(1, -1)
    shift = fading_shift_vector.reshape(1, -1)
    weights = (asker_matrix, matcher_matrix, fading_matrix, content_matrix, result_valve_matrix)

    def local_part(raws, first_slot):
        fade_spec = pl.BlockSpec(
            (rows, heads), lambda i, p: (jnp.bitwise_xor(i + first_slot, p[1]), 0)
        )
        return pl.pallas_call(
            lambda *r: local_kernel(heads, *r),
            grid_spec=pltpu.PrefetchScalarGridSpec(
                num_scalar_prefetch=1,
                grid=(2,),
                in_specs=[pl.BlockSpec(memory_space=pl.ANY)] * 2
                + [whole(mix_gain)]
                + [whole(w) for w in weights]
                + [whole(shift), fade_spec],
                out_specs=[
                    by_slot(rows, value_width),
                    by_slot(rows, key_width),
                    by_slot(rows, value_width),
                    by_slot(pack_rows, key_width),
                ],
                scratch_shapes=[
                    pltpu.VMEM((2, rows, feature_width), bf16),
                    pltpu.SemaphoreType.DMA((2,)),
                ],
            ),
            out_shape=[
                jax.ShapeDtypeStruct((2, rows, value_width), f32),
                jax.ShapeDtypeStruct((2, rows, key_width), bf16),
                jax.ShapeDtypeStruct((2, rows, value_width), bf16),
                jax.ShapeDtypeStruct((2, pack_rows, key_width), f32),
            ],
            compiler_params=params(),
            cost_estimate=cost(1e10, 1e7),
        )(place, *raws, mix_gain, *weights, shift, extra_fade_amount)

    *part_a, pack_a = local_part((mixer_microbatch, mix_raw_c), 0)
    *part_b, pack_b = local_part((mix_raw_x, mix_raw_xc), 2)
    pack_shape = jax.ShapeDtypeStruct((pack_rows, key_width), bf16)

    def small_call(kernel, ins):
        return pl.pallas_call(
            kernel,
            in_specs=smem + vmem(len(ins)),
            out_specs=pl.BlockSpec(memory_space=pltpu.VMEM),
            out_shape=pack_shape,
            compiler_params=params(),
            cost_estimate=cost(1e9, 1e6),
        )(place, *ins)

    pack = small_call(lambda *r: chain_kernel(tp_count, *r), (pack_a, pack_b))
    got = lax.ppermute(pack, "ep", [(e, e ^ 1) for e in range(ep_count)])
    pair = small_call(pair_kernel, (pack, got))
    packs = [
        lax.ppermute(pair, "ep", [(e, e + 2 * s) for e in range(ep_count - 2 * s)])
        for s in range(1, ep_count // 2)
    ]
    start = starting_memory.T
    head_gain = subspace_gain_vector.reshape(1, -1)

    def gated_part(part, first_slot):
        ins = (head_gain, start, pack_a, pack_b, got, *packs)
        return pl.pallas_call(
            lambda *r: gated_kernel(heads, tp_count, first_slot, *r),
            grid_spec=pltpu.PrefetchScalarGridSpec(
                num_scalar_prefetch=1,
                grid=(2,),
                in_specs=[
                    by_slot(rows, value_width),
                    by_slot(rows, key_width),
                    by_slot(rows, value_width),
                ]
                + [whole(a) for a in ins],
                out_specs=[pl.BlockSpec((rows, value_width), lambda i, p: (0, 0))] * 2,
                scratch_shapes=[pltpu.VMEM((tp_count, value_width, key_width), bf16)],
            ),
            out_shape=[jax.ShapeDtypeStruct((rows, value_width), bf16)] * 2,
            compiler_params=params(),
            cost_estimate=cost(2e9, 6e6),
        )(place, *part, *ins)

    gated_b = gated_part(part_b, 2)
    gated_a = gated_part(part_a, 0)
    gated = [*gated_a, *gated_b]
    per_token = [gated[0]] + [
        lax.ppermute(gated[n], "tp", [(t, t ^ n) for t in range(tp_count)])
        for n in range(1, tp_count)
    ]

    near_x = lax.ppermute(near_in, "tp", across)
    shared_mine, shared_other = ffn([normed, normed_x], joint_weights, None, 1)
    shared_back = lax.ppermute(shared_other, "tp", across)
    near_mine, near_other = ffn([near_in, near_x], expert_weights, 0, 2)
    near_back = lax.ppermute(near_other, "tp", across)
    near_sum = pl.pallas_call(
        sum_kernel,
        in_specs=vmem(2),
        out_specs=vmem(ep_count),
        out_shape=[piece] * ep_count,
        compiler_params=params(),
        cost_estimate=cost(1e9, 3e6),
        name="near_sum",
    )(near_mine, near_back)
    near_ret = swap(near_sum)
    far_mine, far_other = ffn([far_in], expert_weights, 1, 2, slots)
    far_back = lax.ppermute(far_other, "tp", across)
    far_sum = pl.pallas_call(
        sum_kernel,
        in_specs=vmem(2),
        out_specs=pl.BlockSpec(memory_space=pltpu.VMEM),
        out_shape=jax.ShapeDtypeStruct((near, feature_width), bf16),
        compiler_params=params(),
        cost_estimate=cost(1e9, 3e6),
        name="far_sum",
    )(far_mine, far_back)
    far_ret = exchange(far_sum)
    (moe_out,) = column_split(
        finish_kernel,
        (near_weight, far_weight, shared_mine, shared_back, far_ret, *near_ret),
        (False, False, True, True, True) + (True,) * ep_count,
        [jax.ShapeDtypeStruct((tokens, feature_width), bf16)],
        2,
        8 * tokens * near * feature_width,
    )

    columns = 4
    out_width = result_matrix.shape[1]
    mixer_sublayer_result = pl.pallas_call(
        lambda *r: project_kernel(tp_count, *r),
        grid=(columns,),
        in_specs=smem
        + [pl.BlockSpec((rows, value_width), lambda i: (0, 0))] * tp_count
        + [
            pl.BlockSpec((result_matrix.shape[0], out_width // columns), lambda i: (0, i)),
        ],
        out_specs=pl.BlockSpec((rows, out_width // columns), lambda i: (0, i)),
        out_shape=jax.ShapeDtypeStruct((rows, out_width), bf16),
        compiler_params=params(),
        cost_estimate=cost(2 * rows * out_width * result_matrix.shape[0], 1e7),
        name="result_project",
    )(tp_place, *per_token, result_matrix)
    return (mixer_sublayer_result, moe_out)


def solution(mesh):
    return jax.shard_map(
        body,
        mesh=mesh,
        in_specs=(
            P(("ep", "tp"), None),
            P(),
            P(None, "tp"),
            P(None, "tp"),
            P(None, "tp"),
            P(None, "tp"),
            P(None, "tp"),
            P("tp"),
            P("ep", "tp"),
            P("tp", None),
            P("tp"),
            P(),
            P(("ep", "tp"), None),
            P(),
            P(("ep", "tp"), None),
            P(("ep", "tp"), None),
            P("ep", None, "tp"),
            P("ep", None, "tp"),
            P("ep", "tp", None),
            P(None, "tp"),
            P(None, "tp"),
            P("tp", None),
        ),
        out_specs=(P(("ep", "tp"), None), P(("ep", "tp"), None)),
        check_vma=False,
    )
```

```python
import jax
import jax.numpy as jnp
from jax import lax
from jax.experimental import pallas as pl
from jax.experimental.pallas import tpu as pltpu
from jax.sharding import PartitionSpec as P

MATCHER_WIDTH = 64
DV = 128
SPAN_LENGTH = 64

NORM_EPS = 1e-06
GATE_SOFTNESS = 16.0
f32 = jnp.float32
bf16 = jnp.bfloat16


def params(mib=None):
    return pltpu.CompilerParams(vmem_limit_bytes=None if mib is None else mib * 1024 * 1024)


def cost(flops, nbytes):
    return pl.CostEstimate(flops=int(flops), bytes_accessed=int(nbytes), transcendentals=0)


def vmem(count):
    return [pl.BlockSpec(memory_space=pltpu.VMEM)] * count


def dot(a, b, dims=((1,), (0,))):
    return lax.dot_general(a, b, (dims, ((), ())), preferred_element_type=f32)


def rms_rows(values, gain):
    widened = values.astype(f32)
    inverse_rms = lax.rsqrt(jnp.mean(widened * widened, axis=-1, keepdims=True) + NORM_EPS)
    return (widened * inverse_rms * gain).astype(bf16)


def silu(v):
    return v * jax.nn.sigmoid(v)


def split_two(v):
    high = v.astype(bf16)
    return high, (v - high.astype(f32)).astype(bf16)


def split_three(v):
    high = v.astype(bf16)
    rest = v - high.astype(f32)
    mid = rest.astype(bf16)
    return high, mid, (rest - mid.astype(f32)).astype(bf16)


def slot_choice(picks, factors, slot_expert, slot_place, experts):
    top, tokens = picks.shape
    slots = slot_expert.shape[0]
    index = lax.broadcasted_iota(jnp.int32, (experts, tokens), 0).astype(f32)
    named = jnp.zeros((experts, tokens), f32)
    weight = jnp.zeros((experts, tokens), f32)
    for k in range(top):
        hit = picks[k : k + 1, :] == index
        named = named + jnp.where(hit, 1.0, 0.0)
        weight = weight + jnp.where(hit, factors[k : k + 1, :], 0.0)
    row = lax.broadcasted_iota(jnp.int32, (tokens, tokens), 0)
    column = lax.broadcasted_iota(jnp.int32, (tokens, tokens), 1)
    earlier = jnp.where(row < column, 1.0, 0.0).astype(bf16)
    rank = dot(named.astype(bf16), earlier)
    spread = lax.broadcasted_iota(jnp.int32, (slots, experts), 1).astype(f32) == slot_expert
    spread = jnp.where(spread, 1.0, 0.0).astype(bf16)
    named_at = dot(spread, named.astype(bf16))
    rank_at = dot(spread, rank.astype(bf16))
    w1, w2, w3 = split_three(weight)
    weight_at = dot(spread, w1) + dot(spread, w2) + dot(spread, w3)
    chosen = (named_at > 0.5) & (rank_at == slot_place)
    return jnp.where(chosen, 1.0, 0.0).astype(bf16), jnp.where(chosen, weight_at, 0.0)


def row_blocks(rows, slots, groups):
    row = lax.broadcasted_iota(jnp.int32, (rows, 1), 0)
    block = jnp.zeros(row.shape, jnp.int32)
    for n in range(1, groups):
        block = block + jnp.where(row >= n * slots, 1, 0)
    return row, block


def pack_own_kernel(
    experts, slots, groups, place_ref, x_ref, gain_ref, picks_ref, factor_ref, *outs
):
    normed_ref, weight_ref, out_ref = outs
    normed = rms_rows(x_ref[...], gain_ref[...])
    normed_ref[...] = normed
    row, block = row_blocks(weight_ref.shape[0], slots, groups)
    local = experts // groups
    place = (row - block * slots).astype(f32)
    picks, factors = picks_ref[...].astype(f32), factor_ref[...]
    pick, _ = slot_choice(picks, factors, (block * local).astype(f32), place, experts)
    owner = jnp.bitwise_xor(block, place_ref[0])
    _, weights = slot_choice(picks, factors, (owner * local).astype(f32), place, experts)
    out_ref[...] = dot(pick, normed).astype(bf16)
    weight_ref[...] = weights


def pack_both_kernel(
    experts,
    slots,
    groups,
    own_ref,
    x_ref,
    gain_ref,
    picks_ref,
    factor_ref,
    picks_x_ref,
    factor_x_ref,
    tok_ref,
    out_ref,
    weight_ref,
):
    tok_ref[...] = rms_rows(x_ref[...], gain_ref[...])
    row, block = row_blocks(weight_ref.shape[0], slots, groups)
    local = experts // groups
    tables = ((block * local + 1).astype(f32), (row - block * slots).astype(f32))
    own, weights = slot_choice(picks_ref[...].astype(f32), factor_ref[...], *tables, experts)
    other, _ = slot_choice(picks_x_ref[...].astype(f32), factor_x_ref[...], *tables, experts)
    weight_ref[...] = weights
    rows = (dot(own, own_ref[...]).astype(bf16), dot(other, tok_ref[...]).astype(bf16))
    for n in range(groups):
        for k in range(2):
            out_ref[(2 * n + k) * slots : (2 * n + k + 1) * slots] = rows[k][
                n * slots : (n + 1) * slots
            ]


def ffn_kernel(arrays, expert, slots, *refs):
    ins = refs[:arrays]
    weights = refs[arrays : arrays + 6]
    outs = refs[arrays + 6 :]
    height = ins[0].shape[0]
    rows = jnp.concatenate([r[...] for r in ins], axis=0)
    total = None
    for n in range(2):
        gate_w, up_w, down_w = (
            w[...] if len(w.shape) == 2 else w[expert] for w in weights[3 * n : 3 * n + 3]
        )
        hidden = (silu(dot(rows, gate_w)) * dot(rows, up_w)).astype(bf16)
        part = dot(hidden, down_w)
        total = part if total is None else total + part
    if len(outs) == arrays:
        for k in range(arrays):
            outs[k][...] = total[k * height : (k + 1) * height].astype(bf16)
        return
    for n in range(height // (2 * slots)):
        for k in range(2):
            piece = total[(2 * n + k) * slots : (2 * n + k + 1) * slots].astype(bf16)
            outs[k][n * slots : (n + 1) * slots] = piece


def ffn(rows, weights, expert, slots=None, grant=None):
    arrays = len(rows)
    count, width = rows[0].shape
    inner = weights[0].shape[-1]
    outs = 2
    out = jax.ShapeDtypeStruct((arrays * count // outs, width), bf16)
    held = expert
    if grant is None and expert is not None:
        held = 0
        weight_specs = [
            pl.BlockSpec((1,) + w.shape[1:], lambda i: (expert, 0, 0)) for w in weights
        ]
    else:
        weight_specs = vmem(6)
    return pl.pallas_call(
        lambda *refs: ffn_kernel(arrays, held, slots, *refs),
        grid=(1,),
        in_specs=vmem(arrays) + weight_specs,
        out_specs=vmem(outs),
        out_shape=[out] * outs,
        compiler_params=params(grant),
        cost_estimate=cost(
            12 * arrays * count * width * inner, 4 * arrays * count * width + 12 * width * inner
        ),
    )(*rows, *weights)


def sum_kernel(a_ref, b_ref, out_ref):
    out_ref[...] = (a_ref[...].astype(f32) + b_ref[...].astype(f32)).astype(bf16)


def sum_swap_kernel(slots, place_ref, a_ref, b_ref, *outs):
    total = (a_ref[...].astype(f32) + b_ref[...].astype(f32)).astype(bf16)
    rows = total.shape[0]
    row, block = row_blocks(rows, slots, len(outs))
    wanted = jnp.bitwise_xor(block, place_ref[0]) * slots + row - block * slots
    column = lax.broadcasted_iota(jnp.int32, (rows, rows), 1)
    pick = jnp.where(column == wanted, 1.0, 0.0).astype(bf16)
    total = dot(pick, total).astype(bf16)
    for n, ref in enumerate(outs):
        ref[...] = total[n * slots : (n + 1) * slots]


def finish_kernel(near_weight_ref, far_weight_ref, shared_ref, got_ref, far_ref, *refs):
    out_ref = refs[-1]
    total = shared_ref[...].astype(f32) + got_ref[...].astype(f32)
    near = jnp.concatenate([r[...] for r in refs[:-1]], axis=0)
    for weight_ref, ret in ((near_weight_ref, near), (far_weight_ref, far_ref[...])):
        for part in split_two(weight_ref[...]):
            total = total + dot(part, ret, ((0,), (0,)))
    out_ref[...] = total.astype(bf16)


def column_split(kernel, ins, blocked, outs, steps, flops):
    specs = []
    for a, cut in zip(ins, blocked):
        lead = a.shape[:-1]
        zeros = (0,) * len(lead)
        if cut:
            specs.append(pl.BlockSpec(lead + (a.shape[-1] // steps,), lambda i, z=zeros: z + (i,)))
        else:
            specs.append(pl.BlockSpec(a.shape, lambda i, z=zeros: z + (0,)))
    out_specs = [
        pl.BlockSpec(o.shape[:-1] + (o.shape[-1] // steps,), lambda i: (0, i)) for o in outs
    ]
    return pl.pallas_call(
        kernel,
        grid=(steps,),
        in_specs=specs,
        out_specs=out_specs,
        out_shape=outs,
        compiler_params=params(12),
        cost_estimate=cost(flops, sum(a.size * a.dtype.itemsize for a in ins)),
    )(*ins)


def local_kernel(heads, carried, place_ref, first_ref, second_ref, *refs):
    gain_ref, shift_ref, fade_ref = refs[:3]
    weight_refs = refs[3:8]
    out_ref, qg_ref, gate_ref, pack_ref = refs[8 + carried : 12 + carried]
    buffer, sems = refs[12 + carried :]
    d_ref, k_ref, q_ref, v_ref, g_ref = weight_refs
    slot = pl.program_id(0)
    span = SPAN_LENGTH
    key_width = q_ref.shape[1]
    value_width = v_ref.shape[1]

    @pl.when(slot == 0)
    def _():
        for n, ref in enumerate((first_ref, second_ref)):
            pltpu.make_async_copy(ref, buffer.at[n], sems.at[n]).start()

    pltpu.make_async_copy(first_ref, buffer.at[slot], sems.at[slot]).wait()
    normed = rms_rows(buffer[slot], gain_ref[...])
    rows = normed.shape[0]
    logits = dot(normed, d_ref[...]).astype(bf16).astype(f32) + shift_ref[...]
    keys = dot(normed, k_ref[...]).astype(bf16).astype(f32)
    query = dot(normed, q_ref[...]).astype(bf16).astype(f32) * MATCHER_WIDTH ** (-0.5)
    value = dot(normed, v_ref[...]).astype(bf16)
    gate_ref[0] = dot(normed, g_ref[...]).astype(bf16)

    head_row = lax.broadcasted_iota(jnp.int32, (heads, key_width), 0)
    head_lane = lax.broadcasted_iota(jnp.int32, (heads, key_width), 1)
    low = head_row * MATCHER_WIDTH
    spread = jnp.where((head_lane >= low) & (head_lane < low + MATCHER_WIDTH), 1.0, 0.0).astype(bf16)
    fade = sum(dot(part, spread, ((0,), (0,))) for part in split_three(fade_ref[...]))
    soft = jnp.minimum(logits, 0.0) - jnp.log1p(jnp.exp(-jnp.abs(logits)))
    rate = soft / GATE_SOFTNESS + fade

    row = lax.broadcasted_iota(jnp.int32, (rows, rows), 0)
    column = lax.broadcasted_iota(jnp.int32, (rows, rows), 1)
    span_bits = span.bit_length() - 1
    same_span = jnp.right_shift(row, span_bits) == jnp.right_shift(column, span_bits)
    lower = jnp.where(same_span & (row >= column), 1.0, 0.0).astype(bf16)
    r1, r2, r3 = split_three(rate)
    running = dot(lower, r1) + dot(lower, r2) + dot(lower, r3)
    query_faded = query * jnp.exp(running)
    key_decayed = (keys * jnp.exp(-running)).astype(bf16)

    width_bits = MATCHER_WIDTH.bit_length() - 1
    value_bits = DV.bit_length() - 1
    lane_head = jnp.right_shift(
        lax.broadcasted_iota(jnp.int32, (span, key_width), 1), width_bits
    )
    causal = (
        jnp.bitwise_and(lax.broadcasted_iota(jnp.int32, (heads * span, span), 0), span - 1)
        >= lax.broadcasted_iota(jnp.int32, (heads * span, span), 1)
    )
    own_block = jnp.right_shift(
        lax.broadcasted_iota(jnp.int32, (value_width, key_width), 0), value_bits
    ) == jnp.right_shift(lax.broadcasted_iota(jnp.int32, (value_width, key_width), 1), width_bits)

    held = jnp.zeros((value_width, key_width), f32)
    passed = jnp.zeros((1, key_width), f32)
    for n in range(rows // span):
        at = slice(n * span, (n + 1) * span)
        qf = query_faded[at]
        total = running[(n + 1) * span - 1 : (n + 1) * span]
        qb = qf.astype(bf16)
        vb = value[at]
        key_end = (keys[at] * jnp.exp(total - running[at])).astype(bf16)
        stacked = jnp.concatenate(
            [jnp.where(lane_head == h, qf, 0.0) for h in range(heads)], axis=0
        ).astype(bf16)
        scores = dot(stacked, key_decayed[at], ((1,), (1,)))
        scores = jnp.where(causal, scores, 0.0).astype(bf16)
        inner = jnp.concatenate(
            [
                dot(scores[h * span : (h + 1) * span], vb[:, h * DV : (h + 1) * DV])
                for h in range(heads)
            ],
            axis=1,
        )
        outer = dot(qb, held.astype(bf16), ((1,), (1,)))
        out_ref[0, at, :] = inner + outer
        qg_ref[0, at, :] = (qf * jnp.exp(passed)).astype(bf16)
        added = dot(vb, key_end, ((0,), (0,)))
        held = held * jnp.exp(total) + jnp.where(own_block, added, 0.0)
        passed = passed + total
    compact = held[0:DV]
    for h in range(1, heads):
        compact = compact + held[h * DV : (h + 1) * DV]
    pack_ref[0, 0:DV, :] = compact
    pack_ref[0, DV:, :] = jnp.broadcast_to(
        jnp.exp(passed), (pack_ref.shape[1] - DV, key_width)
    )


def follow(held, pack):
    return held * pack[DV : DV + 1].astype(f32) + pack[0:DV].astype(f32)


def chain_kernel(blocks, place_ref, packs_ref, out_ref):
    held = None
    for n in range(blocks):
        pack = packs_ref[jnp.bitwise_xor(place_ref[1], n)]
        if held is None:
            held, fading = pack[0:DV], pack[DV : DV + 1]
        else:
            held, fading = follow(held, pack), fading * pack[DV : DV + 1]
    held = held.astype(bf16)
    fading = jnp.broadcast_to(fading, (out_ref.shape[1] - DV, fading.shape[1])).astype(bf16)
    for n in range(out_ref.shape[0]):
        out_ref[n, 0:DV, :] = held
        out_ref[n, DV:, :] = fading


def gated_kernel(
    heads,
    blocks,
    place_ref,
    local_ref,
    qg_ref,
    gate_ref,
    gain_ref,
    start_ref,
    block_ref,
    pack_ref,
    *refs,
):
    outs = refs[:-1]
    entering = refs[-1]
    key_width = qg_ref.shape[2]

    @pl.when(pl.program_id(0) == 0)
    def _():
        held = start_ref[...].T
        for n in range(pack_ref.shape[0]):
            held = jnp.where(place_ref[0] > n, follow(held, pack_ref[n]), held)
        width_bits = MATCHER_WIDTH.bit_length() - 1
        lane_head = jnp.right_shift(
            lax.broadcasted_iota(jnp.int32, (DV, key_width), 1), width_bits
        )
        for n in range(blocks):
            slot = jnp.bitwise_xor(place_ref[1], n)
            for h in range(heads):
                entering[slot, h * DV : (h + 1) * DV, :] = jnp.where(
                    lane_head == h, held, 0.0
                ).astype(bf16)
            held = follow(held, block_ref[slot])

    slot = jnp.bitwise_xor(pl.program_id(0), blocks // 2)
    attended = local_ref[0] + dot(qg_ref[0], entering[slot], ((1,), (1,)))
    parts = []
    for h in range(heads):
        at = slice(h * DV, (h + 1) * DV)
        part = attended[:, at]
        inverse = lax.rsqrt(jnp.mean(part * part, axis=-1, keepdims=True) + NORM_EPS)
        part = part * inverse * gain_ref[:, at] * silu(gate_ref[0, :, at].astype(f32))
        parts.append(part.astype(bf16))
    rows = jnp.concatenate(parts, axis=1)
    for n, ref in enumerate(outs):

        @pl.when(slot == n)
        def _(ref=ref):
            ref[...] = rows


def project_kernel(place_ref, first_ref, second_ref, *refs):
    weights = refs[0:2]
    out_ref = refs[-1]
    total = dot(first_ref[...], weights[0][...]) + dot(second_ref[...], weights[1][...])
    if len(refs) == 4:
        total = total + refs[2][...]
    out_ref[...] = total.astype(out_ref.dtype)


def body(
    mixer_microbatch,
    mixer_gain_vector,
    asker_matrix,
    matcher_matrix,
    fading_matrix,
    content_matrix,
    result_valve_matrix,
    fading_shift_vector,
    extra_fade_amount,
    starting_memory,
    subspace_gain_vector,
    result_matrix,
    specialist_microbatch,
    specialist_gain_vector,
    picked_specialists,
    specialist_mixing_factor,
    specialist_valve_matrix,
    specialist_widen_matrix,
    specialist_shrink_matrix,
    joint_valve_matrix,
    joint_widen_matrix,
    joint_shrink_matrix,
):
    ep_count = lax.axis_size("ep")
    tp_count = lax.axis_size("tp")
    across = [(t, t ^ 2) for t in range(tp_count)]
    beside = [(t, t ^ 1) for t in range(tp_count)]
    ep_place = lax.axis_index("ep").astype(jnp.int32).reshape(1)
    tp_place = lax.axis_index("tp").astype(jnp.int32).reshape(1)

    tokens, feature_width = specialist_microbatch.shape
    top_count = picked_specialists.shape[1]
    local_experts = specialist_widen_matrix.shape[0]
    if local_experts != 2 or tp_count != 4:
        raise ValueError("unsupported sizes")
    experts = local_experts * ep_count
    slots = max(2, 3 * tokens * top_count // (2 * experts))

    picks, factors = picked_specialists.T, specialist_mixing_factor.T
    moe_raw_x = lax.ppermute(specialist_microbatch, "tp", across)
    picks_x = lax.ppermute(picks, "tp", across)
    factors_x = lax.ppermute(factors, "tp", across)
    mix_raw_x = lax.ppermute(mixer_microbatch, "tp", across)
    mix_raw_c = lax.ppermute(mixer_microbatch, "tp", beside)
    mix_raw_xc = lax.ppermute(mix_raw_x, "tp", beside)
    joint_weights = (joint_valve_matrix, joint_widen_matrix, joint_shrink_matrix)
    joint_weights += tuple(lax.ppermute(w, "tp", beside) for w in joint_weights)
    expert_weights = (specialist_valve_matrix, specialist_widen_matrix, specialist_shrink_matrix)
    expert_weights += tuple(lax.ppermute(w, "tp", beside) for w in expert_weights)

    near = ep_count * slots
    far = 2 * near
    moe_gain = specialist_gain_vector.reshape(1, -1)
    piece = jax.ShapeDtypeStruct((slots, feature_width), bf16)
    smem = [pl.BlockSpec(memory_space=pltpu.SMEM)]
    normed, near_weight, near_out = pl.pallas_call(
        lambda *r: pack_own_kernel(experts, slots, ep_count, *r),
        in_specs=smem + vmem(4),
        out_specs=vmem(3),
        out_shape=[
            jax.ShapeDtypeStruct((tokens, feature_width), bf16),
            jax.ShapeDtypeStruct((near, tokens), f32),
            jax.ShapeDtypeStruct((near, feature_width), bf16),
        ],
        compiler_params=params(),
        cost_estimate=cost(2e9, 4e6),
        name="pack_own",
    )(ep_place, specialist_microbatch, moe_gain, picks, factors)

    def swap(pieces):
        return [pieces[0]] + [
            lax.ppermute(pieces[n], "ep", [(e, e ^ n) for e in range(ep_count)])
            for n in range(1, ep_count)
        ]

    def exchange(rows):
        shape = rows.shape
        cut = rows.reshape(ep_count, shape[0] // ep_count, shape[1])
        out = lax.all_to_all(cut, "ep", split_axis=0, concat_axis=0, tiled=True)
        return out.reshape(shape)

    near_in = exchange(near_out)

    normed_x, far_out, far_weight = pl.pallas_call(
        lambda *r: pack_both_kernel(experts, slots, ep_count, *r),
        in_specs=vmem(7),
        out_specs=vmem(3),
        out_shape=[
            jax.ShapeDtypeStruct((tokens, feature_width), bf16),
            jax.ShapeDtypeStruct((far, feature_width), bf16),
            jax.ShapeDtypeStruct((near, tokens), f32),
        ],
        compiler_params=params(),
        cost_estimate=cost(3e9, 6e6),
        name="pack_both",
    )(
        normed,
        moe_raw_x,
        moe_gain,
        picks,
        factors,
        picks_x,
        factors_x,
    )
    far_in = exchange(far_out)

    rows = mixer_microbatch.shape[0]
    key_width = asker_matrix.shape[1]
    value_width = content_matrix.shape[1]
    heads = value_width // DV
    pack_rows = DV + 16
    place = jnp.concatenate([ep_place, tp_place])
    whole = lambda a: pl.BlockSpec(a.shape, lambda i, *_: (0,) * len(a.shape))
    mix_gain = mixer_gain_vector.reshape(1, -1)
    shift = fading_shift_vector.reshape(1, -1)
    weights = (fading_matrix, matcher_matrix, asker_matrix, content_matrix, result_valve_matrix)
    fade = extra_fade_amount.T
    any_space = pl.BlockSpec(memory_space=pl.ANY)

    def local_part(raws, first_slot, carried=()):
        fade_spec = pl.BlockSpec(
            (heads, rows), lambda i, p: (0, jnp.bitwise_xor(i + first_slot, p[1]))
        )
        by_slot = lambda r, w: pl.BlockSpec((1, r, w), lambda i, p: (i + first_slot, 0, 0))
        shapes = [
            jax.ShapeDtypeStruct((tp_count, rows, value_width), f32),
            jax.ShapeDtypeStruct((tp_count, rows, key_width), bf16),
            jax.ShapeDtypeStruct((tp_count, rows, value_width), bf16),
            jax.ShapeDtypeStruct((tp_count, pack_rows, key_width), f32),
        ]
        return pl.pallas_call(
            lambda *r: local_kernel(heads, len(carried), *r),
            grid_spec=pltpu.PrefetchScalarGridSpec(
                num_scalar_prefetch=1,
                grid=(2,),
                in_specs=[any_space] * 2
                + [whole(mix_gain), whole(shift), fade_spec]
                + vmem(5)
                + [any_space] * len(carried),
                out_specs=[by_slot(*shape.shape[1:]) for shape in shapes],
                scratch_shapes=[
                    pltpu.VMEM((2, rows, feature_width), bf16),
                    pltpu.SemaphoreType.DMA((2,)),
                ],
            ),
            out_shape=shapes,
            input_output_aliases={11 + n: n for n in range(len(carried))},
            compiler_params=params(),
            cost_estimate=cost(1e10, 1e7),
        )(place, *raws, mix_gain, shift, fade, *weights, *carried)

    local = local_part((mixer_microbatch, mix_raw_c), 0)
    *local, block_packs = local_part((mix_raw_x, mix_raw_xc), 2, local)
    pack = pl.pallas_call(
        lambda *r: chain_kernel(tp_count, *r),
        in_specs=smem + vmem(1),
        out_specs=pl.BlockSpec(memory_space=pltpu.VMEM),
        out_shape=jax.ShapeDtypeStruct((ep_count, pack_rows, key_width), bf16),
        compiler_params=params(),
        cost_estimate=cost(1e9, 1e6),
        name="chain_state",
    )(place, block_packs)
    packs = lax.all_to_all(pack, "ep", split_axis=0, concat_axis=0, tiled=True)
    head_gain = subspace_gain_vector.reshape(1, -1)
    by_turn = lambda r, w: pl.BlockSpec(
        (1, r, w), lambda i, p: (jnp.bitwise_xor(i, tp_count // 2), 0, 0)
    )
    ins = (head_gain, starting_memory, block_packs, packs)
    gated = pl.pallas_call(
        lambda *r: gated_kernel(heads, tp_count, *r),
        grid_spec=pltpu.PrefetchScalarGridSpec(
            num_scalar_prefetch=1,
            grid=(tp_count,),
            in_specs=[by_turn(*a.shape[1:]) for a in local] + [whole(a) for a in ins],
            out_specs=[pl.BlockSpec((rows, value_width), lambda i, p: (0, 0))] * tp_count,
            scratch_shapes=[pltpu.VMEM((tp_count, value_width, key_width), bf16)],
        ),
        out_shape=[jax.ShapeDtypeStruct((rows, value_width), bf16)] * tp_count,
        compiler_params=params(),
        cost_estimate=cost(2e9, 6e6),
        name="gated_heads",
    )(place, *local, *ins)
    per_token = [gated[0]] + [
        lax.ppermute(gated[n], "tp", [(t, t ^ n) for t in range(tp_count)])
        for n in range(1, tp_count)
    ]

    near_x = lax.ppermute(near_in, "tp", across)
    shared_mine, shared_other = ffn([normed, normed_x], joint_weights, None)
    shared_back = lax.ppermute(shared_other, "tp", across)
    near_mine, near_other = ffn([near_in, near_x], expert_weights, 0)
    near_back = lax.ppermute(near_other, "tp", across)
    near_sum = pl.pallas_call(
        lambda *r: sum_swap_kernel(slots, *r),
        in_specs=smem + vmem(2),
        out_specs=vmem(ep_count),
        out_shape=[piece] * ep_count,
        compiler_params=params(),
        cost_estimate=cost(1e9, 3e6),
        name="near_sum",
    )(ep_place, near_mine, near_back)
    near_ret = swap(near_sum)
    far_mine, far_other = ffn([far_in], expert_weights, 1, slots)
    far_back = lax.ppermute(far_other, "tp", across)
    far_sum = pl.pallas_call(
        sum_kernel,
        in_specs=vmem(2),
        out_specs=pl.BlockSpec(memory_space=pltpu.VMEM),
        out_shape=jax.ShapeDtypeStruct((near, feature_width), bf16),
        compiler_params=params(),
        cost_estimate=cost(1e9, 3e6),
        name="far_sum",
    )(far_mine, far_back)
    far_ret = exchange(far_sum)
    (moe_out,) = column_split(
        finish_kernel,
        (near_weight, far_weight, shared_mine, shared_back, far_ret, *near_ret),
        (False, False, True, True, True) + (True,) * ep_count,
        [jax.ShapeDtypeStruct((tokens, feature_width), bf16)],
        2,
        8 * tokens * near * feature_width,
    )

    out_width = result_matrix.shape[1]
    columns = out_width // 2

    def project(first, kind, before=()):
        weight_specs = [
            pl.BlockSpec(
                (value_width, columns), lambda i, p, n=n: (jnp.bitwise_xor(p[1], n), i)
            )
            for n in (first, first + 1)
        ]
        out_spec = pl.BlockSpec((rows, columns), lambda i, p: (0, i))
        return pl.pallas_call(
            project_kernel,
            grid_spec=pltpu.PrefetchScalarGridSpec(
                num_scalar_prefetch=1,
                grid=(2,),
                in_specs=[pl.BlockSpec((rows, value_width), lambda i, p: (0, 0))] * 2
                + weight_specs
                + [out_spec] * len(before),
                out_specs=out_spec,
            ),
            out_shape=jax.ShapeDtypeStruct((rows, out_width), kind),
            compiler_params=params(),
            cost_estimate=cost(rows * out_width * result_matrix.shape[0], 5e6),
        )(place, *per_token[first : first + 2], result_matrix, result_matrix, *before)

    partial = project(0, f32)
    mixer_sublayer_result = project(2, bf16, (partial,))
    return (mixer_sublayer_result, moe_out)


def solution(mesh):
    return jax.shard_map(
        body,
        mesh=mesh,
        in_specs=(
            P(("ep", "tp"), None),
            P(),
            P(None, "tp"),
            P(None, "tp"),
            P(None, "tp"),
            P(None, "tp"),
            P(None, "tp"),
            P("tp"),
            P("ep", "tp"),
            P("tp", None),
            P("tp"),
            P(),
            P(("ep", "tp"), None),
            P(),
            P(("ep", "tp"), None),
            P(("ep", "tp"), None),
            P("ep", None, "tp"),
            P("ep", None, "tp"),
            P("ep", "tp", None),
            P(None, "tp"),
            P(None, "tp"),
            P("tp", None),
        ),
        out_specs=(P(("ep", "tp"), None), P(("ep", "tp"), None)),
        check_vma=False,
    )
```

```python
import jax
import jax.numpy as jnp
from jax import lax
from jax.experimental import pallas as pl
from jax.experimental.pallas import tpu as pltpu
from jax.sharding import PartitionSpec as P

MATCHER_WIDTH = 64
DV = 128
SPAN_LENGTH = 64

NORM_EPS = 1e-06
GATE_SOFTNESS = 16.0
f32 = jnp.float32
bf16 = jnp.bfloat16


def params(mib=None):
    return pltpu.CompilerParams(vmem_limit_bytes=None if mib is None else mib * 1024 * 1024)


def cost(flops, nbytes):
    return pl.CostEstimate(flops=int(flops), bytes_accessed=int(nbytes), transcendentals=0)


def vmem(count):
    return [pl.BlockSpec(memory_space=pltpu.VMEM)] * count


def dot(a, b, dims=((1,), (0,))):
    return lax.dot_general(a, b, (dims, ((), ())), preferred_element_type=f32)


def rms_rows(values, gain):
    widened = values.astype(f32)
    inverse_rms = lax.rsqrt(jnp.mean(widened * widened, axis=-1, keepdims=True) + NORM_EPS)
    return (widened * inverse_rms * gain).astype(bf16)


def silu(v):
    return v * jax.nn.sigmoid(v)


def split_two(v):
    high = v.astype(bf16)
    return high, (v - high.astype(f32)).astype(bf16)


def split_three(v):
    high = v.astype(bf16)
    rest = v - high.astype(f32)
    mid = rest.astype(bf16)
    return high, mid, (rest - mid.astype(f32)).astype(bf16)


def slot_choice(picks, factors, slot_expert, slot_place, experts):
    top, tokens = picks.shape
    slots = slot_expert.shape[0]
    index = lax.broadcasted_iota(jnp.int32, (experts, tokens), 0).astype(f32)
    named = jnp.zeros((experts, tokens), f32)
    weight = jnp.zeros((experts, tokens), f32)
    for k in range(top):
        hit = picks[k : k + 1, :] == index
        named = named + jnp.where(hit, 1.0, 0.0)
        weight = weight + jnp.where(hit, factors[k : k + 1, :], 0.0)
    row = lax.broadcasted_iota(jnp.int32, (tokens, tokens), 0)
    column = lax.broadcasted_iota(jnp.int32, (tokens, tokens), 1)
    earlier = jnp.where(row < column, 1.0, 0.0).astype(bf16)
    rank = dot(named.astype(bf16), earlier)
    spread = lax.broadcasted_iota(jnp.int32, (slots, experts), 1).astype(f32) == slot_expert
    spread = jnp.where(spread, 1.0, 0.0).astype(bf16)
    named_at = dot(spread, named.astype(bf16))
    rank_at = dot(spread, rank.astype(bf16))
    w1, w2, w3 = split_three(weight)
    weight_at = dot(spread, w1) + dot(spread, w2) + dot(spread, w3)
    chosen = (named_at > 0.5) & (rank_at == slot_place)
    return jnp.where(chosen, 1.0, 0.0).astype(bf16), jnp.where(chosen, weight_at, 0.0)


def row_blocks(rows, slots, groups):
    row = lax.broadcasted_iota(jnp.int32, (rows, 1), 0)
    block = jnp.zeros(row.shape, jnp.int32)
    for n in range(1, groups):
        block = block + jnp.where(row >= n * slots, 1, 0)
    return row, block


def pack_own_kernel(
    experts, slots, groups, place_ref, x_ref, gain_ref, picks_ref, factor_ref, *outs
):
    normed_ref, weight_ref, out_ref = outs
    normed = rms_rows(x_ref[...], gain_ref[...])
    normed_ref[...] = normed
    row, block = row_blocks(weight_ref.shape[0], slots, groups)
    local = experts // groups
    place = (row - block * slots).astype(f32)
    picks, factors = picks_ref[...].astype(f32), factor_ref[...]
    pick, _ = slot_choice(picks, factors, (block * local).astype(f32), place, experts)
    owner = jnp.bitwise_xor(block, place_ref[0])
    _, weights = slot_choice(picks, factors, (owner * local).astype(f32), place, experts)
    out_ref[...] = dot(pick, normed).astype(bf16)
    weight_ref[...] = weights


def pack_both_kernel(
    experts,
    slots,
    groups,
    own_ref,
    x_ref,
    gain_ref,
    picks_ref,
    factor_ref,
    picks_x_ref,
    factor_x_ref,
    tok_ref,
    out_ref,
    weight_ref,
):
    tok_ref[...] = rms_rows(x_ref[...], gain_ref[...])
    row, block = row_blocks(weight_ref.shape[0], slots, groups)
    local = experts // groups
    tables = ((block * local + 1).astype(f32), (row - block * slots).astype(f32))
    own, weights = slot_choice(picks_ref[...].astype(f32), factor_ref[...], *tables, experts)
    other, _ = slot_choice(picks_x_ref[...].astype(f32), factor_x_ref[...], *tables, experts)
    weight_ref[...] = weights
    rows = (dot(own, own_ref[...]).astype(bf16), dot(other, tok_ref[...]).astype(bf16))
    for n in range(groups):
        for k in range(2):
            out_ref[(2 * n + k) * slots : (2 * n + k + 1) * slots] = rows[k][
                n * slots : (n + 1) * slots
            ]


def ffn_kernel(arrays, held, slots, *refs):
    ins = refs[:arrays]
    weights = [w[held] if len(w.shape) == 3 else w[...] for w in refs[arrays : arrays + 6]]
    outs = refs[arrays + 6 :]
    height = ins[0].shape[0]
    rows = jnp.concatenate([r[...] for r in ins], axis=0)
    gate = dot(rows, jnp.concatenate([weights[0], weights[3]], axis=1))
    up = dot(rows, jnp.concatenate([weights[1], weights[4]], axis=1))
    hidden = (silu(gate) * up).astype(bf16)
    total = dot(hidden, jnp.concatenate([weights[2], weights[5]], axis=0))
    if len(outs) == arrays:
        for k in range(arrays):
            outs[k][...] = total[k * height : (k + 1) * height].astype(bf16)
        return
    for n in range(height // (2 * slots)):
        for k in range(2):
            piece = total[(2 * n + k) * slots : (2 * n + k + 1) * slots].astype(bf16)
            outs[k][n * slots : (n + 1) * slots] = piece


def ffn(rows, weights, expert, slots=None, grant=None, whole=False):
    arrays = len(rows)
    count, width = rows[0].shape
    inner = weights[0].shape[-1]
    outs = 2
    out = jax.ShapeDtypeStruct((arrays * count // outs, width), bf16)
    held = 0
    if expert is None or whole:
        held, weight_specs = expert, vmem(6)
    else:
        weight_specs = [
            pl.BlockSpec((1,) + w.shape[1:], lambda i: (expert, 0, 0)) for w in weights
        ]
    return pl.pallas_call(
        lambda *refs: ffn_kernel(arrays, held, slots, *refs),
        grid=(1,),
        in_specs=vmem(arrays) + weight_specs,
        out_specs=vmem(outs),
        out_shape=[out] * outs,
        compiler_params=params(grant),
        cost_estimate=cost(
            12 * arrays * count * width * inner, 4 * arrays * count * width + 12 * width * inner
        ),
    )(*rows, *weights)


def sum_kernel(a_ref, b_ref, out_ref):
    out_ref[...] = (a_ref[...].astype(f32) + b_ref[...].astype(f32)).astype(bf16)


def sum_swap_kernel(slots, place_ref, a_ref, b_ref, *outs):
    total = (a_ref[...].astype(f32) + b_ref[...].astype(f32)).astype(bf16)
    rows = total.shape[0]
    row, block = row_blocks(rows, slots, len(outs))
    wanted = jnp.bitwise_xor(block, place_ref[0]) * slots + row - block * slots
    column = lax.broadcasted_iota(jnp.int32, (rows, rows), 1)
    pick = jnp.where(column == wanted, 1.0, 0.0).astype(bf16)
    total = dot(pick, total).astype(bf16)
    for n, ref in enumerate(outs):
        ref[...] = total[n * slots : (n + 1) * slots]


def finish_kernel(near_weight_ref, far_weight_ref, shared_ref, got_ref, far_ref, *refs):
    out_ref = refs[-1]
    total = shared_ref[...].astype(f32) + got_ref[...].astype(f32)
    near = jnp.concatenate([r[...] for r in refs[:-1]], axis=0)
    for weight_ref, ret in ((near_weight_ref, near), (far_weight_ref, far_ref[...])):
        for part in split_two(weight_ref[...]):
            total = total + dot(part, ret, ((0,), (0,)))
    out_ref[...] = total.astype(bf16)


def column_split(kernel, ins, blocked, outs, steps, flops):
    specs = []
    for a, cut in zip(ins, blocked):
        lead = a.shape[:-1]
        zeros = (0,) * len(lead)
        if cut:
            specs.append(pl.BlockSpec(lead + (a.shape[-1] // steps,), lambda i, z=zeros: z + (i,)))
        else:
            specs.append(pl.BlockSpec(a.shape, lambda i, z=zeros: z + (0,)))
    out_specs = [
        pl.BlockSpec(o.shape[:-1] + (o.shape[-1] // steps,), lambda i: (0, i)) for o in outs
    ]
    return pl.pallas_call(
        kernel,
        grid=(steps,),
        in_specs=specs,
        out_specs=out_specs,
        out_shape=outs,
        compiler_params=params(12),
        cost_estimate=cost(flops, sum(a.size * a.dtype.itemsize for a in ins)),
    )(*ins)


def local_kernel(heads, carried, place_ref, first_ref, second_ref, *refs):
    gain_ref, shift_ref, fade_ref = refs[:3]
    weight_refs = refs[3:8]
    out_ref, qg_ref, gate_ref, pack_ref = refs[8 + carried : 12 + carried]
    buffer, *held_weights, sems, weight_sems = refs[12 + carried :]
    d_ref, k_ref, q_ref, v_ref, g_ref = held_weights
    slot = pl.program_id(0)
    span = SPAN_LENGTH
    key_width = q_ref.shape[1]
    value_width = v_ref.shape[1]
    fetches = [
        pltpu.make_async_copy(weight_refs[n], held_weights[n], weight_sems.at[n])
        for n in range(5)
    ]

    @pl.when(slot == 0)
    def _():
        pltpu.make_async_copy(first_ref, buffer.at[0], sems.at[0]).start()
        for fetch in fetches:
            fetch.start()
        pltpu.make_async_copy(second_ref, buffer.at[1], sems.at[1]).start()

    def ready(*which):
        @pl.when(slot == 0)
        def _():
            for n in which:
                fetches[n].wait()

    pltpu.make_async_copy(first_ref, buffer.at[slot], sems.at[slot]).wait()
    ready(0, 1, 2, 3, 4)
    normed = rms_rows(buffer[slot], gain_ref[...])
    rows = normed.shape[0]
    logits = dot(normed, d_ref[...]).astype(bf16).astype(f32) + shift_ref[...]
    keys = dot(normed, k_ref[...]).astype(bf16).astype(f32)
    query = dot(normed, q_ref[...]).astype(bf16).astype(f32) * MATCHER_WIDTH ** (-0.5)
    value = dot(normed, v_ref[...]).astype(bf16)
    gate_ref[0] = dot(normed, g_ref[...]).astype(bf16)

    head_row = lax.broadcasted_iota(jnp.int32, (heads, key_width), 0)
    head_lane = lax.broadcasted_iota(jnp.int32, (heads, key_width), 1)
    low = head_row * MATCHER_WIDTH
    spread = jnp.where((head_lane >= low) & (head_lane < low + MATCHER_WIDTH), 1.0, 0.0).astype(bf16)
    fade = sum(dot(part, spread, ((0,), (0,))) for part in split_three(fade_ref[...]))
    soft = jnp.minimum(logits, 0.0) - jnp.log1p(jnp.exp(-jnp.abs(logits)))
    rate = soft / GATE_SOFTNESS + fade

    row = lax.broadcasted_iota(jnp.int32, (rows, rows), 0)
    column = lax.broadcasted_iota(jnp.int32, (rows, rows), 1)
    span_bits = span.bit_length() - 1
    same_span = jnp.right_shift(row, span_bits) == jnp.right_shift(column, span_bits)
    lower = jnp.where(same_span & (row >= column), 1.0, 0.0).astype(bf16)
    r1, r2, r3 = split_three(rate)
    running = dot(lower, r1) + dot(lower, r2) + dot(lower, r3)
    query_faded = query * jnp.exp(running)
    key_decayed = (keys * jnp.exp(-running)).astype(bf16)

    width_bits = MATCHER_WIDTH.bit_length() - 1
    value_bits = DV.bit_length() - 1
    lane_head = jnp.right_shift(
        lax.broadcasted_iota(jnp.int32, (span, key_width), 1), width_bits
    )
    causal = (
        jnp.bitwise_and(lax.broadcasted_iota(jnp.int32, (heads * span, span), 0), span - 1)
        >= lax.broadcasted_iota(jnp.int32, (heads * span, span), 1)
    )
    own_block = jnp.right_shift(
        lax.broadcasted_iota(jnp.int32, (value_width, key_width), 0), value_bits
    ) == jnp.right_shift(lax.broadcasted_iota(jnp.int32, (value_width, key_width), 1), width_bits)

    held = jnp.zeros((value_width, key_width), f32)
    passed = jnp.zeros((1, key_width), f32)
    for n in range(rows // span):
        at = slice(n * span, (n + 1) * span)
        qf = query_faded[at]
        total = running[(n + 1) * span - 1 : (n + 1) * span]
        qb = qf.astype(bf16)
        vb = value[at]
        key_end = (keys[at] * jnp.exp(total - running[at])).astype(bf16)
        stacked = jnp.concatenate(
            [jnp.where(lane_head == h, qf, 0.0) for h in range(heads)], axis=0
        ).astype(bf16)
        scores = dot(stacked, key_decayed[at], ((1,), (1,)))
        scores = jnp.where(causal, scores, 0.0).astype(bf16)
        inner = jnp.concatenate(
            [
                dot(scores[h * span : (h + 1) * span], vb[:, h * DV : (h + 1) * DV])
                for h in range(heads)
            ],
            axis=1,
        )
        outer = dot(qb, held.astype(bf16), ((1,), (1,)))
        out_ref[0, at, :] = (inner + outer).astype(bf16)
        qg_ref[0, at, :] = (qf * jnp.exp(passed)).astype(bf16)
        added = dot(vb, key_end, ((0,), (0,)))
        held = held * jnp.exp(total) + jnp.where(own_block, added, 0.0)
        passed = passed + total
    compact = held[0:DV]
    for h in range(1, heads):
        compact = compact + held[h * DV : (h + 1) * DV]
    pack_ref[0, 0:DV, :] = compact
    pack_ref[0, DV:, :] = jnp.broadcast_to(
        jnp.exp(passed), (pack_ref.shape[1] - DV, key_width)
    )


def follow(held, pack):
    return held * pack[DV : DV + 1].astype(f32) + pack[0:DV].astype(f32)


def chain_kernel(blocks, of_tp, place_ref, packs_ref, out_ref):
    held = None
    for n in range(blocks):
        pack = packs_ref[jnp.bitwise_xor(of_tp(place_ref), n)]
        if held is None:
            held, fading = pack[0:DV], pack[DV : DV + 1]
        else:
            held, fading = follow(held, pack), fading * pack[DV : DV + 1]
    held = held.astype(bf16)
    fading = jnp.broadcast_to(fading, (out_ref.shape[1] - DV, fading.shape[1])).astype(bf16)
    for n in range(out_ref.shape[0]):
        out_ref[n, 0:DV, :] = held
        out_ref[n, DV:, :] = fading


def gated_kernel(
    heads,
    blocks,
    of_ep,
    of_tp,
    place_ref,
    local_ref,
    qg_ref,
    gate_ref,
    gain_ref,
    start_ref,
    block_ref,
    pack_ref,
    *refs,
):
    outs = refs[:-1]
    entering = refs[-1]
    key_width = qg_ref.shape[2]

    @pl.when(pl.program_id(0) == 0)
    def _():
        held = start_ref[...].T
        for n in range(pack_ref.shape[0]):
            held = jnp.where(of_ep(place_ref) > n, follow(held, pack_ref[n]), held)
        width_bits = MATCHER_WIDTH.bit_length() - 1
        lane_head = jnp.right_shift(
            lax.broadcasted_iota(jnp.int32, (DV, key_width), 1), width_bits
        )
        for n in range(blocks):
            slot = jnp.bitwise_xor(of_tp(place_ref), n)
            for h in range(heads):
                entering[slot, h * DV : (h + 1) * DV, :] = jnp.where(
                    lane_head == h, held, 0.0
                ).astype(bf16)
            held = follow(held, block_ref[slot])

    slot = jnp.bitwise_xor(pl.program_id(0), blocks // 2)
    attended = local_ref[0].astype(f32) + dot(qg_ref[0], entering[slot], ((1,), (1,)))
    parts = []
    for h in range(heads):
        at = slice(h * DV, (h + 1) * DV)
        part = attended[:, at]
        inverse = lax.rsqrt(jnp.mean(part * part, axis=-1, keepdims=True) + NORM_EPS)
        part = part * inverse * gain_ref[:, at] * silu(gate_ref[0, :, at].astype(f32))
        parts.append(part.astype(bf16))
    rows = jnp.concatenate(parts, axis=1)
    for n, ref in enumerate(outs):

        @pl.when(slot == n)
        def _(ref=ref):
            ref[...] = rows


def project_kernel(place_ref, first_ref, second_ref, *refs):
    weights = refs[0:2]
    out_ref = refs[-1]
    total = dot(first_ref[...], weights[0][...]) + dot(second_ref[...], weights[1][...])
    if len(refs) == 4:
        total = total + refs[2][...]
    out_ref[...] = total.astype(out_ref.dtype)


def body(
    mixer_microbatch,
    mixer_gain_vector,
    asker_matrix,
    matcher_matrix,
    fading_matrix,
    content_matrix,
    result_valve_matrix,
    fading_shift_vector,
    extra_fade_amount,
    starting_memory,
    subspace_gain_vector,
    result_matrix,
    specialist_microbatch,
    specialist_gain_vector,
    picked_specialists,
    specialist_mixing_factor,
    specialist_valve_matrix,
    specialist_widen_matrix,
    specialist_shrink_matrix,
    joint_valve_matrix,
    joint_widen_matrix,
    joint_shrink_matrix,
):
    ep_count = lax.axis_size("ep")
    tp_count = lax.axis_size("tp")
    across = [(t, t ^ 2) for t in range(tp_count)]
    beside = [(t, t ^ 1) for t in range(tp_count)]
    ep_place = lax.axis_index("ep").astype(jnp.int32).reshape(1)
    tp_place = lax.axis_index("tp").astype(jnp.int32).reshape(1)
    place = ep_place * tp_count + tp_place
    tp_bits = tp_count.bit_length() - 1
    of_tp = lambda p: jnp.bitwise_and(p[0], tp_count - 1)
    of_ep = lambda p: jnp.right_shift(p[0], tp_bits)

    tokens, feature_width = specialist_microbatch.shape
    top_count = picked_specialists.shape[1]
    local_experts = specialist_widen_matrix.shape[0]
    if local_experts != 2 or tp_count != 4:
        raise ValueError("unsupported sizes")
    experts = local_experts * ep_count
    slots = max(2, 3 * tokens * top_count // (2 * experts))

    picks, factors = picked_specialists.T, specialist_mixing_factor.T
    moe_raw_x = lax.ppermute(specialist_microbatch, "tp", across)
    picks_x = lax.ppermute(picks, "tp", across)
    factors_x = lax.ppermute(factors, "tp", across)
    mix_raw_x = lax.ppermute(mixer_microbatch, "tp", across)
    mix_raw_c = lax.ppermute(mixer_microbatch, "tp", beside)
    mix_raw_xc = lax.ppermute(mix_raw_x, "tp", beside)
    joint_weights = (joint_valve_matrix, joint_widen_matrix, joint_shrink_matrix)
    joint_weights += tuple(lax.ppermute(w, "tp", beside) for w in joint_weights)
    expert_weights = (specialist_valve_matrix, specialist_widen_matrix, specialist_shrink_matrix)
    expert_weights += tuple(lax.ppermute(w, "tp", beside) for w in expert_weights)

    near = ep_count * slots
    far = 2 * near
    moe_gain = specialist_gain_vector.reshape(1, -1)
    piece = jax.ShapeDtypeStruct((slots, feature_width), bf16)
    smem = [pl.BlockSpec(memory_space=pltpu.SMEM)]
    normed, near_weight, near_out = pl.pallas_call(
        lambda *r: pack_own_kernel(experts, slots, ep_count, *r),
        in_specs=smem + vmem(4),
        out_specs=vmem(3),
        out_shape=[
            jax.ShapeDtypeStruct((tokens, feature_width), bf16),
            jax.ShapeDtypeStruct((near, tokens), f32),
            jax.ShapeDtypeStruct((near, feature_width), bf16),
        ],
        compiler_params=params(),
        cost_estimate=cost(2e9, 4e6),
        name="pa",
    )(ep_place, specialist_microbatch, moe_gain, picks, factors)

    def swap(pieces):
        out = [pieces[0]]
        for n in range(1, ep_count):
            pairs = [(e, e ^ n) for e in range(ep_count)]
            out.append(lax.ppermute(pieces[n], "ep", pairs))
        return out

    def exchange(rows):
        shape = rows.shape
        cut = rows.reshape(ep_count, shape[0] // ep_count, shape[1])
        out = lax.all_to_all(cut, "ep", split_axis=0, concat_axis=0, tiled=True)
        return out.reshape(shape)

    near_in = exchange(near_out)

    normed_x, far_out, far_weight = pl.pallas_call(
        lambda *r: pack_both_kernel(experts, slots, ep_count, *r),
        in_specs=vmem(7),
        out_specs=vmem(3),
        out_shape=[
            jax.ShapeDtypeStruct((tokens, feature_width), bf16),
            jax.ShapeDtypeStruct((far, feature_width), bf16),
            jax.ShapeDtypeStruct((near, tokens), f32),
        ],
        compiler_params=params(63),
        cost_estimate=cost(3e9, 6e6),
        name="pb",
    )(
        normed,
        moe_raw_x,
        moe_gain,
        picks,
        factors,
        picks_x,
        factors_x,
    )
    far_in = exchange(far_out)

    rows = mixer_microbatch.shape[0]
    key_width = asker_matrix.shape[1]
    value_width = content_matrix.shape[1]
    heads = value_width // DV
    pack_rows = DV + 16
    whole = lambda a: pl.BlockSpec(a.shape, lambda i, *_: (0,) * len(a.shape))
    mix_gain = mixer_gain_vector.reshape(1, -1)
    shift = fading_shift_vector.reshape(1, -1)
    weights = (fading_matrix, matcher_matrix, asker_matrix, content_matrix, result_valve_matrix)
    fade = extra_fade_amount.T
    any_space = pl.BlockSpec(memory_space=pl.ANY)

    def local_part(raws, first_slot, carried=()):
        fade_spec = pl.BlockSpec(
            (heads, rows), lambda i, p: (0, jnp.bitwise_xor(i + first_slot, of_tp(p)))
        )
        by_slot = lambda r, w: pl.BlockSpec((1, r, w), lambda i, p: (i + first_slot, 0, 0))
        shapes = [
            jax.ShapeDtypeStruct((tp_count, rows, value_width), bf16),
            jax.ShapeDtypeStruct((tp_count, rows, key_width), bf16),
            jax.ShapeDtypeStruct((tp_count, rows, value_width), bf16),
            jax.ShapeDtypeStruct((tp_count, pack_rows, key_width), f32),
        ]
        return pl.pallas_call(
            lambda *r: local_kernel(heads, len(carried), *r),
            grid_spec=pltpu.PrefetchScalarGridSpec(
                num_scalar_prefetch=1,
                grid=(2,),
                in_specs=[any_space] * 2
                + [whole(mix_gain), whole(shift), fade_spec]
                + [any_space] * (5 + len(carried)),
                out_specs=[by_slot(*shape.shape[1:]) for shape in shapes],
                scratch_shapes=[
                    pltpu.VMEM((2, rows, feature_width), bf16),
                    *[pltpu.VMEM(w.shape, bf16) for w in weights],
                    pltpu.SemaphoreType.DMA((2,)),
                    pltpu.SemaphoreType.DMA((5,)),
                ],
            ),
            out_shape=shapes,
            input_output_aliases={11 + n: n for n in range(len(carried))},
            compiler_params=params(),
            cost_estimate=cost(1e10, 1e7),
        )(place, *raws, mix_gain, shift, fade, *weights, *carried)

    local = local_part((mixer_microbatch, mix_raw_c), 0)
    *local, block_packs = local_part((mix_raw_x, mix_raw_xc), 2, local)
    pack = pl.pallas_call(
        lambda *r: chain_kernel(tp_count, of_tp, *r),
        in_specs=smem + vmem(1),
        out_specs=pl.BlockSpec(memory_space=pltpu.VMEM),
        out_shape=jax.ShapeDtypeStruct((ep_count, pack_rows, key_width), bf16),
        compiler_params=params(),
        cost_estimate=cost(1e9, 1e6),
        name="chain",
    )(place, block_packs)
    packs = lax.all_to_all(pack, "ep", split_axis=0, concat_axis=0, tiled=True)
    head_gain = subspace_gain_vector.reshape(1, -1)
    by_turn = lambda r, w: pl.BlockSpec(
        (1, r, w), lambda i, p: (jnp.bitwise_xor(i, tp_count // 2), 0, 0)
    )
    ins = (head_gain, starting_memory, block_packs, packs)
    gated = pl.pallas_call(
        lambda *r: gated_kernel(heads, tp_count, of_ep, of_tp, *r),
        grid_spec=pltpu.PrefetchScalarGridSpec(
            num_scalar_prefetch=1,
            grid=(tp_count,),
            in_specs=[by_turn(*a.shape[1:]) for a in local] + [whole(a) for a in ins],
            out_specs=[pl.BlockSpec((rows, value_width), lambda i, p: (0, 0))] * tp_count,
            scratch_shapes=[pltpu.VMEM((tp_count, value_width, key_width), bf16)],
        ),
        out_shape=[jax.ShapeDtypeStruct((rows, value_width), bf16)] * tp_count,
        compiler_params=params(),
        cost_estimate=cost(2e9, 6e6),
        name="gated",
    )(place, *local, *ins)
    per_token = [gated[0]] + [
        lax.ppermute(gated[n], "tp", [(t, t ^ n) for t in range(tp_count)])
        for n in range(1, tp_count)
    ]

    near_x = lax.ppermute(near_in, "tp", across)
    shared_mine, shared_other = ffn([normed, normed_x], joint_weights, None, grant=16)
    shared_back = lax.ppermute(shared_other, "tp", across)
    near_mine, near_other = ffn([near_in, near_x], expert_weights, 0)
    near_back = lax.ppermute(near_other, "tp", across)
    near_sum = pl.pallas_call(
        lambda *r: sum_swap_kernel(slots, *r),
        in_specs=smem + vmem(2),
        out_specs=vmem(ep_count),
        out_shape=[piece] * ep_count,
        compiler_params=params(),
        cost_estimate=cost(1e9, 3e6),
        name="nsum",
    )(ep_place, near_mine, near_back)
    near_ret = swap(near_sum)
    far_mine, far_other = ffn([far_in], expert_weights, 1, slots)
    far_back = lax.ppermute(far_other, "tp", across)
    far_sum = pl.pallas_call(
        sum_kernel,
        in_specs=vmem(2),
        out_specs=pl.BlockSpec(memory_space=pltpu.VMEM),
        out_shape=jax.ShapeDtypeStruct((near, feature_width), bf16),
        compiler_params=params(),
        cost_estimate=cost(1e9, 3e6),
        name="fsum",
    )(far_mine, far_back)
    far_ret = exchange(far_sum)
    (moe_out,) = column_split(
        finish_kernel,
        (near_weight, far_weight, shared_mine, shared_back, far_ret, *near_ret),
        (False, False, True, True, True) + (True,) * ep_count,
        [jax.ShapeDtypeStruct((tokens, feature_width), bf16)],
        2,
        8 * tokens * near * feature_width,
    )

    out_width = result_matrix.shape[1]
    columns = out_width // 2

    def project(first, kind, before=()):
        weight_specs = [
            pl.BlockSpec(
                (value_width, columns), lambda i, p, n=n: (jnp.bitwise_xor(of_tp(p), n), i)
            )
            for n in (first, first + 1)
        ]
        out_spec = pl.BlockSpec((rows, columns), lambda i, p: (0, i))
        return pl.pallas_call(
            project_kernel,
            grid_spec=pltpu.PrefetchScalarGridSpec(
                num_scalar_prefetch=1,
                grid=(2,),
                in_specs=[pl.BlockSpec((rows, value_width), lambda i, p: (0, 0))] * 2
                + weight_specs
                + [out_spec] * len(before),
                out_specs=out_spec,
            ),
            out_shape=jax.ShapeDtypeStruct((rows, out_width), kind),
            compiler_params=params(),
            cost_estimate=cost(rows * out_width * result_matrix.shape[0], 5e6),
        )(place, *per_token[first : first + 2], result_matrix, result_matrix, *before)

    partial = project(0, f32)
    mixer_sublayer_result = project(2, bf16, (partial,))
    return (mixer_sublayer_result, moe_out)


def solution(mesh):
    return jax.shard_map(
        body,
        mesh=mesh,
        in_specs=(
            P(("ep", "tp"), None),
            P(),
            P(None, "tp"),
            P(None, "tp"),
            P(None, "tp"),
            P(None, "tp"),
            P(None, "tp"),
            P("tp"),
            P("ep", "tp"),
            P("tp", None),
            P("tp"),
            P(),
            P(("ep", "tp"), None),
            P(),
            P(("ep", "tp"), None),
            P(("ep", "tp"), None),
            P("ep", None, "tp"),
            P("ep", None, "tp"),
            P("ep", "tp", None),
            P(None, "tp"),
            P(None, "tp"),
            P("tp", None),
        ),
        out_specs=(P(("ep", "tp"), None), P(("ep", "tp"), None)),
        check_vma=False,
    )
```
